32 devices in a mesh: ep: 8 (over z, x), tp: 4 (over y, core).
Axes of the slice: x: 2, y: 2, z: 4, core: 2. Of those that a mesh axis runs over, the one named last changes fastest.
Arguments:
- out_gate: bfloat16 [8192, 1024], P('ep', 'tp'), may hold values from -6 to 6
- in_gate: bfloat16 [8192, 1024], P('ep', 'tp'), may hold values from -6 to 6
- conv_input: bfloat16 [8192, 1024], P('ep', 'tp'), may hold values from -6 to 6
- conv_taps: float32 [3, 1024], P(None, 'tp'), may hold values from -4 to 4
- group_gain: float32 [1024], P('tp'), may hold values from 0.1 to 1.9
- mix_out_w: bfloat16 [1024, 2048], replicated, may hold values from -0.1875 to 0.1875
- moe_in: bfloat16 [8192, 2048], P(('ep', 'tp')), may hold values from -6 to 6
- moe_gain: float32 [2048], replicated, may hold values from 0.1 to 1.9
- route_ids: int32 [8192, 2], P(('ep', 'tp')), may hold values from 0 to 31, as said below
- route_weight: float32 [8192, 2], P(('ep', 'tp')), may hold values from 0.1 to 1
- gate_w: bfloat16 [32, 2048, 1024], P(('ep', 'tp')), may hold values from -0.125 to 0.125
- up_w: bfloat16 [32, 2048, 1024], P(('ep', 'tp')), may hold values from -0.125 to 0.125
- down_w: bfloat16 [32, 1024, 2048], P(('ep', 'tp')), may hold values from -0.1875 to 0.1875
Outputs:
- mixed: bfloat16 [8192, 2048], P(('ep', 'tp'))
- moe_out: bfloat16 [8192, 2048], P(('ep', 'tp'))
The draws below stay inside these ranges and needn't reach their ends.
Inputs may be any that keep to these rules, and one draw needn't show every extreme that they name: `route_ids`: the two numbers of a row are different experts of one group: group g holds experts g * 4 to g * 4 + 3. The rows of one device (aligned blocks of 256 rows) name each group in exactly 32 rows and each expert in exactly 16 rows.
All inputs are finite; a program needn't handle non-finite values.
Results may differ from the reference program's by a relative error of at most 0.0071.
Values may be sent and summed in bfloat16 or wider, within the bound.
A program may use at most 128 MiB of HBM per device.

```python
import jax
import jax.numpy as jnp
from jax import lax

D = 2048
CC = 1024
GROUP_CH = 64
TAPS = 3
FE = 1024
TOK_B = 256
GROUPS = 8
EXP_GROUP = 4
EXPERTS = 32
TOKENS_A = 8192
TOKENS_B = 8192


def draw_route_ids(key, part):
    block_count = TOKENS_B // TOK_B
    per_group = TOK_B // GROUPS
    block_keys = jax.random.split(jax.random.fold_in(key, 11), block_count)

    def one_block(block_key):
        order_key, label_key = jax.random.split(block_key)
        slot_of = jax.random.permutation(order_key, TOK_B).astype(jnp.int32)
        group_of = slot_of // per_group
        inner_slot = slot_of % per_group
        first_pick = inner_slot % EXP_GROUP
        shift_by = 1 + inner_slot // EXP_GROUP % (EXP_GROUP - 1)
        second_pick = (first_pick + shift_by) % EXP_GROUP
        label_keys = jax.random.split(label_key, GROUPS)
        labels = jax.vmap(lambda one_key: jax.random.permutation(one_key, EXP_GROUP))(label_keys).astype(jnp.int32)
        first_id = group_of * EXP_GROUP + labels[group_of, first_pick]
        second_id = group_of * EXP_GROUP + labels[group_of, second_pick]
        return jnp.stack([first_id, second_id], axis=1)
    return jax.vmap(one_block)(block_keys).reshape(TOKENS_B, 2).astype(jnp.int32)


def block_scale(own_key, extent, cuts, low, largest):
    loudness, own = 1.0, jax.random.fold_in(own_key, 6)
    for dim, parts in cuts:
        draws = jnp.exp(jax.random.uniform(jax.random.fold_in(own, dim), (parts,), jnp.float32, low / len(cuts), largest / len(cuts)))
        loudness = loudness * jnp.repeat(draws, extent[dim] // parts).reshape([-1 if axis == dim else 1 for axis in range(len(extent))])
    return loudness


def centred(own_key, shape, deviation, bound, pieces=(), dtype=jnp.bfloat16):
    drawn = deviation * jax.random.normal(own_key, shape, jnp.float32)
    if pieces:
        drawn = drawn * block_scale(own_key, shape, pieces, -0.22, 0.18)
    return jnp.clip(drawn, -bound, bound).astype(dtype)


def setup_inputs(seed: int = 0) -> dict:
    keys = jax.random.split(jax.random.key(seed), 14)
    return {
        "out_gate": centred(keys[0], (TOKENS_A, CC), 1.0, 6.0, ((0, 8), (1, 4))),
        "in_gate": centred(keys[1], (TOKENS_A, CC), 1.0, 6.0, ((0, 8), (1, 4))),
        "conv_input": centred(keys[2], (TOKENS_A, CC), 1.0, 6.0, ((0, 8), (1, 4))),
        "conv_taps": centred(keys[3], (TAPS, CC), 0.577, 4.0, ((1, 4),), jnp.float32),
        "group_gain": jnp.clip(1.0 + 0.18 * jax.random.normal(keys[4], (CC,), jnp.float32), 0.1, 1.9),
        "mix_out_w": centred(keys[5], (CC, D), CC ** -0.5, 0.1875),
        "moe_in": centred(keys[6], (TOKENS_B, D), 1.0, 6.0, ((0, 32),)),
        "moe_gain": jnp.clip(1.0 + 0.18 * jax.random.normal(keys[7], (D,), jnp.float32), 0.1, 1.9),
        "route_ids": draw_route_ids(jax.random.fold_in(keys[13], 71), 0),
        "route_weight": jnp.clip(0.1 + 0.9 * jax.random.uniform(keys[9], (TOKENS_B, 2), jnp.float32) ** block_scale(keys[9], (TOKENS_B, 2), ((0, 32),), -0.2, 0.2), 0.1, 1.0),
        "gate_w": centred(keys[10], (EXPERTS, D, FE), D ** -0.5, 0.125, ((0, 32),)),
        "up_w": centred(keys[11], (EXPERTS, D, FE), D ** -0.5, 0.125, ((0, 32),)),
        "down_w": centred(keys[12], (EXPERTS, FE, D), FE ** -0.5, 0.1875, ((0, 32),)),
    }


def conv_mixer(out_gate, in_gate, conv_input, conv_taps, group_gain, mix_out_w):
    product = in_gate.astype(jnp.float32) * conv_input.astype(jnp.float32)
    length = product.shape[0]
    padded = jnp.pad(product, ((TAPS - 1, 0), (0, 0)))
    convolved = jnp.zeros_like(product)
    for tap in range(TAPS):
        convolved = convolved + conv_taps[tap] * padded[tap:tap + length]
    gated = out_gate.astype(jnp.float32) * convolved
    grouped = gated.reshape(length, CC // GROUP_CH, GROUP_CH)
    inv_rms = lax.rsqrt(lax.optimization_barrier(jnp.mean(grouped * grouped, axis=-1, keepdims=True)) + 1e-06)
    normed = ((grouped * inv_rms).reshape(length, CC) * group_gain).astype(jnp.bfloat16)
    return jnp.dot(normed, mix_out_w, preferred_element_type=jnp.float32).astype(jnp.bfloat16)

def expert_rows(inputs, w_gate, w_up, w_down):
    gate_part = jnp.dot(inputs, w_gate, preferred_element_type=jnp.float32)
    up_part = jnp.dot(inputs, w_up, preferred_element_type=jnp.float32)
    hidden = (jax.nn.silu(gate_part) * up_part).astype(jnp.bfloat16)
    return jnp.dot(hidden, w_down, preferred_element_type=jnp.float32).astype(jnp.bfloat16)

def reference(out_gate, in_gate, conv_input, conv_taps, group_gain, mix_out_w, moe_in, moe_gain, route_ids, route_weight, gate_w, up_w, down_w):
    mixed = conv_mixer(out_gate, in_gate, conv_input, conv_taps, group_gain, mix_out_w)
    wide_in = moe_in.astype(jnp.float32)
    inv_rms = lax.rsqrt(lax.optimization_barrier(jnp.mean(wide_in * wide_in, axis=-1, keepdims=True)) + 1e-06)
    expert_in = (wide_in * inv_rms * moe_gain).astype(jnp.bfloat16)
    flat_ids = route_ids.reshape(-1).astype(jnp.int32)
    sort_order = jnp.argsort(flat_ids).astype(jnp.int32)
    per_expert = flat_ids.shape[0] // EXPERTS
    tokens_of = (sort_order // 2).reshape(EXPERTS, per_expert)

    def one_expert(operands):
        token_rows, w_gate, w_up, w_down = operands
        return expert_rows(expert_in[token_rows], w_gate, w_up, w_down)
    outputs = lax.map(one_expert, (tokens_of, gate_w, up_w, down_w))
    per_assign = jnp.zeros((flat_ids.shape[0], D), jnp.bfloat16).at[sort_order].set(outputs.reshape(-1, D))
    per_assign = per_assign.reshape(-1, 2, D)
    first_out = per_assign[:, 0].astype(jnp.float32)
    second = per_assign[:, 1].astype(jnp.float32)
    moe_out = (first_out * route_weight[:, 0:1] + second * route_weight[:, 1:2]).astype(jnp.bfloat16)
    return (mixed, moe_out)
```

```python
import functools

import jax
import jax.numpy as jnp
from jax import lax
from jax.experimental import pallas as pl
from jax.experimental.pallas import tpu as pltpu
from jax.sharding import PartitionSpec as P

GROUP_CH = 64
HALO = 16
MESH = pl.DeviceIdType.MESH
BF16 = jnp.bfloat16
F32 = jnp.float32


def round_up(value, to):
    return (value + to - 1) // to * to


def tdot(a, b):
    return lax.dot_general(a, b, (((0,), (0,)), ((), ())), preferred_element_type=F32)


def dot_t(a, b):
    return lax.dot_general(a, b, (((1,), (1,)), ((), ())), preferred_element_type=F32)


def flip(index, mask):
    bit = 1
    out = index
    while bit <= mask:
        if mask & bit:
            out = out + bit * (1 - 2 * ((index // bit) % 2))
        bit *= 2
    return out


def layer_kernel(
    n_ep, n_tp, pad_slot, chunks, reach,
    og_hbm, ig_hbm, ci_hbm, taps_hbm, ggain_hbm, wm_hbm,
    x_hbm, mgain_hbm, ids_hbm, rw_hbm, wg_hbm, wu_hbm, wd_hbm,
    mixed_hbm, fin_hbm, place_hbm,
    og, ig, ci, taps, ggain, wm, x, mgain, ids, rw, wg, wu, wd,
    normed, gated, norm, place, sorted_rows, landed, picked, xin, hidden, comb, sums, fin, mixin, mixed,
    in_sem, out_sem, h_send, h_recv, m_send, m_recv, d_send, d_recv, p_send, p_recv, r_send, r_recv, f_send, f_recv,
):
    me_e = lax.axis_index("ep")
    me_t = lax.axis_index("tp")
    tok, width = x.shape
    rows = tok // n_ep
    slots = n_tp * pad_slot
    experts = n_ep * n_tp
    rows_a, lanes = og.shape
    part = rows_a // n_tp

    barrier = pltpu.get_barrier_semaphore()
    for k in range(1, n_ep):
        pl.semaphore_signal(
            barrier, inc=1, device_id={"ep": flip(me_e, k), "tp": me_t}, device_id_type=MESH
        )
    for j in range(1, n_tp):
        pl.semaphore_signal(
            barrier, inc=1, device_id={"ep": me_e, "tp": flip(me_t, j)}, device_id_type=MESH
        )
    nxt = lax.rem(me_e + 1, n_ep)
    own = pl.ds(HALO, rows_a)
    loads = {}
    for i, (name, src, dst) in enumerate((
        ("ids", ids_hbm, ids), ("rw", rw_hbm, rw), ("mgain", mgain_hbm, mgain), ("x", x_hbm, x),
        ("ig", ig_hbm, ig.at[own]), ("ci", ci_hbm, ci.at[own]), ("og", og_hbm, og),
        ("taps", taps_hbm, taps), ("ggain", ggain_hbm, ggain),
        ("wg", wg_hbm.at[0], wg), ("wu", wu_hbm.at[0], wu), ("wd", wd_hbm.at[0], wd), ("wm", wm_hbm, wm),
    )):
        loads[name] = pltpu.make_async_copy(src, dst, in_sem.at[i])
        loads[name].start()

    loads["ids"].wait()
    loads["rw"].wait()
    ids0, ids1 = ids[0:1, :], ids[1:2, :]
    sub_e = lax.broadcasted_iota(jnp.int32, (experts, tok), 0)
    hit0 = (ids0 == sub_e).astype(F32)
    hit1 = (ids1 == sub_e).astype(F32)
    both = (hit0 + hit1).astype(BF16)
    upper = (
        lax.broadcasted_iota(jnp.int32, (tok, tok), 0) < lax.broadcasted_iota(jnp.int32, (tok, tok), 1)
    ).astype(BF16)
    before = jnp.dot(both, upper, preferred_element_type=F32)
    rank0 = jnp.sum(before * hit0, axis=0, keepdims=True).astype(jnp.int32)
    rank1 = jnp.sum(before * hit1, axis=0, keepdims=True).astype(jnp.int32)
    group = ids0 // n_tp
    in_group = (group == (sub_e // n_tp)).astype(F32)
    rank_g = jnp.sum(before * in_group, axis=0, keepdims=True).astype(jnp.int32) // 2
    place[...] = (
        (group * rows + rank_g) == lax.broadcasted_iota(jnp.int32, (tok, tok), 0)
    ).astype(BF16)
    place_out = pltpu.make_async_copy(place, place_hbm, out_sem.at[0])
    place_out.start()
    cell0 = (ids0 - group * n_tp) * pad_slot + rank0
    cell1 = (ids1 - group * n_tp) * pad_slot + rank1
    sub_s = lax.broadcasted_iota(jnp.int32, (slots, tok), 0)
    weight = jnp.where(cell0 == sub_s, rw[0:1, :], 0.0) + jnp.where(cell1 == sub_s, rw[1:2, :], 0.0)
    high = weight.astype(BF16)
    low = (weight - high.astype(F32)).astype(BF16)
    cells = jnp.concatenate([high, low], axis=0)
    sorted_rows[:, width:] = dot_t(place[...], cells).astype(BF16)

    loads["mgain"].wait()
    loads["x"].wait()
    step = 32

    @pl.loop(0, tok // step)
    def _(i):
        at = pl.ds(pl.multiple_of(i * step, step), step)
        wide = x[at, :].astype(F32)
        scale = lax.rsqrt(jnp.mean(wide * wide, axis=-1, keepdims=True) + 1e-06)
        norm[at, :] = (wide * scale * mgain[...]).astype(BF16)

    @pl.loop(0, width // 512)
    def _(f):
        cols = pl.ds(pl.multiple_of(f * 512, 512), 512)
        sorted_rows[:, cols] = jnp.dot(
            place[...], norm[:, cols], preferred_element_type=F32
        ).astype(BF16)

    pl.semaphore_wait(barrier, n_ep - 1 + n_tp - 1)

    sends = []

    def send(src, dst, s_sem, r_sem, ep, tp):
        copy = pltpu.make_async_remote_copy(
            src_ref=src, dst_ref=dst, send_sem=s_sem, recv_sem=r_sem,
            device_id={"ep": ep, "tp": tp}, device_id_type=MESH,
        )
        copy.start()
        sends.append(copy)
        return copy

    dispatch = {}
    for k in range(1, n_ep):
        to = flip(me_e, k)
        dispatch[k] = send(
            sorted_rows.at[pl.ds(pl.multiple_of(to * rows, rows), rows)],
            landed.at[k], d_send.at[k], d_recv.at[k], to, me_t,
        )
    loads["ig"].wait()
    loads["ci"].wait()
    tail, head = pl.ds(rows_a, HALO), pl.ds(0, HALO)
    halos = [
        send(ref.at[tail], ref.at[head], h_send.at[i], h_recv.at[i], nxt, me_t)
        for i, ref in enumerate((ig, ci))
    ]
    landed[0] = sorted_rows[pl.ds(pl.multiple_of(me_e * rows, rows), rows), :]

    spread = {}

    def scatter(k):
        if k:
            dispatch[k].wait_recv()
        chosen = (landed[k, :, pl.ds(width, slots)].astype(F32) != 0.0).astype(BF16)
        picked[k] = tdot(chosen, landed[k, :, 0:width]).astype(BF16)
        for j in range(n_tp - 1, 0, -1):
            to = flip(me_t, j)
            spread[k, j] = send(
                picked.at[k, pl.ds(pl.multiple_of(to * pad_slot, pad_slot), pad_slot)],
                xin.at[pl.ds((k * n_tp + j) * pad_slot, pad_slot)],
                p_send.at[k, j], p_recv.at[k, j], me_e, to,
            )
        xin[pl.ds(k * n_tp * pad_slot, pad_slot), :] = picked[
            k, pl.ds(pl.multiple_of(me_t * pad_slot, pad_slot), pad_slot), :
        ]

    scatter(0)

    loads["og"].wait()
    loads["taps"].wait()
    loads["ggain"].wait()
    for copy in halos:
        copy.wait_recv()

    @pl.when(me_e == 0)
    def _():
        ig[0:HALO, :] = jnp.zeros((HALO, lanes), BF16)

    same = (
        lax.broadcasted_iota(jnp.int32, (lanes, lanes), 0) // GROUP_CH
        == lax.broadcasted_iota(jnp.int32, (lanes, lanes), 1) // GROUP_CH
    ).astype(BF16)
    own_lanes = pl.ds(pl.multiple_of(me_t * lanes, lanes), lanes)
    mixes = []
    for j in range(n_tp - 1, -1, -1):
        to = flip(me_t, j)
        base = pl.multiple_of(to * part, part)
        cstep = 64

        @pl.loop(0, part // cstep)
        def _(i):
            at = pl.multiple_of(base + i * cstep, cstep)
            span = pl.ds(at, cstep + HALO)
            product = ig[span, :].astype(F32) * ci[span, :].astype(F32)
            total = taps[reach : reach + 1, :] * product[HALO:, :]
            for back_by in range(1, reach + 1):
                total = total + taps[reach - back_by : reach - back_by + 1, :] * (
                    product[HALO - back_by : HALO - back_by + cstep, :]
                )
            gated[pl.ds(pl.multiple_of(i * cstep, cstep), cstep), :] = (
                og[pl.ds(at, cstep), :].astype(F32) * total
            )

        value = gated[...]
        square = value * value
        s_high = square.astype(BF16)
        s_low = (square - s_high.astype(F32)).astype(BF16)
        mean = (
            jnp.dot(s_high, same, preferred_element_type=F32)
            + jnp.dot(s_low, same, preferred_element_type=F32)
        ) * (1.0 / GROUP_CH)
        done = (value * lax.rsqrt(mean + 1e-06) * ggain[...]).astype(BF16)
        if j:
            normed[pl.ds(base, part), :] = done
            mixes.append(send(
                normed.at[pl.ds(base, part)], mixin.at[:, own_lanes],
                m_send.at[j], m_recv.at[j], me_e, to,
            ))
        else:
            mixin[:, own_lanes] = done

    hid = wg.shape[1]
    per = n_ep // chunks
    many = per * slots
    back = {}
    mine = pl.ds(pl.multiple_of(me_t * pad_slot, pad_slot), pad_slot)
    here = pl.ds(pl.multiple_of(me_e * rows, rows), rows)

    def expert(c):
        for k in range(c * per, (c + 1) * per):
            for j in range(1, n_tp):
                spread[k, j].wait_recv()
        span = pl.ds(c * many, many)

        @pl.loop(0, hid // 256)
        def _(f):
            cols = pl.ds(pl.multiple_of(f * 256, 256), 256)
            gate = jnp.dot(xin[span, :], wg[:, cols], preferred_element_type=F32)
            up = jnp.dot(xin[span, :], wu[:, cols], preferred_element_type=F32)
            hidden[:, cols] = (gate / (1.0 + jnp.exp(-gate)) * up).astype(BF16)

        @pl.loop(0, width // 512)
        def _(f):
            cols = pl.ds(pl.multiple_of(f * 512, 512), 512)
            xin[span, cols] = jnp.dot(
                hidden[...], wd[:, cols], preferred_element_type=F32
            ).astype(BF16)

    def give_back(c):
        for k in range(c * per, (c + 1) * per):
            for j in range(n_tp - 1, 0, -1):
                back[k, j] = send(
                    xin.at[pl.ds((k * n_tp + j) * pad_slot, pad_slot)],
                    comb.at[k, mine], r_send.at[k, j], r_recv.at[k, j], me_e, flip(me_t, j),
                )
            comb[k, mine, :] = xin[pl.ds(k * slots, pad_slot), :]

    home = {}

    def combine(k):
        for j in range(1, n_tp):
            back[k, j].wait_recv()
        total = jnp.dot(
            landed[k, :, pl.ds(width, slots)], comb[k], preferred_element_type=F32
        ) + jnp.dot(
            landed[k, :, pl.ds(width + slots, slots)], comb[k], preferred_element_type=F32
        )
        if k == 0:
            fin[here, :] = total.astype(BF16)
            return
        sums[k] = total.astype(BF16)
        home[k] = send(sums.at[k], fin.at[here], f_send.at[k], f_recv.at[k], flip(me_e, k), me_t)

    half = n_ep // 2
    near = list(range(chunks // 2))
    far = list(range(chunks // 2, chunks))
    for k in range(1, half):
        scatter(k)
    for name in ("wg", "wu", "wd", "wm"):
        loads[name].wait()
    expert(near[0])
    scatter(half)
    for c in near[1:]:
        expert(c)
    scatter(half + 1)
    for copy in mixes:
        copy.wait_recv()

    @pl.loop(0, width // 512)
    def _(f):
        cols = pl.ds(pl.multiple_of(f * 512, 512), 512)
        mixed[:, cols] = jnp.dot(mixin[...], wm[:, cols], preferred_element_type=F32).astype(BF16)

    mixed_out = pltpu.make_async_copy(mixed, mixed_hbm, out_sem.at[1])
    mixed_out.start()
    for k in range(half + 2, n_ep):
        scatter(k)
    for c in far:
        expert(c)
        give_back(c)
    for c in near[::-1]:
        give_back(c)
    order = [k for c in far + near[::-1] for k in range(c * per, (c + 1) * per)]
    for k in order:
        combine(k)
    fin_out = []

    def finish(k):
        block = pl.ds(pl.multiple_of(flip(me_e, k) * rows, rows), rows)
        copy = pltpu.make_async_copy(fin.at[block], fin_hbm.at[block], out_sem.at[2 + k])
        copy.start()
        fin_out.append(copy)

    for k in order:
        if k:
            home[k].wait_recv()
        finish(k)
    for copy in sends:
        copy.wait_send()
    for copy in [place_out, mixed_out] + fin_out:
        copy.wait()


def layer(
    out_gate, in_gate, conv_input, conv_taps, group_gain, mix_out_w,
    moe_in, moe_gain, route_ids, route_weight, gate_w, up_w, down_w,
):
    n_ep, n_tp = lax.axis_size("ep"), lax.axis_size("tp")
    tok, width = moe_in.shape
    hid = gate_w.shape[2]
    pad_slot = round_up(2 * tok // (n_ep * n_tp), 16)
    rows = tok // n_ep
    slots = n_tp * pad_slot
    meta = round_up(2 * slots, 128)
    total = n_ep * slots
    chunks = 4
    rows_a, lanes = out_gate.shape
    part = rows_a // n_tp
    channels = mix_out_w.shape[0]
    taps = conv_taps.shape[0]
    hbm = pl.BlockSpec(memory_space=pl.ANY)
    dma = pltpu.SemaphoreType.DMA
    vm = pltpu.VMEM
    return pl.pallas_call(
        functools.partial(layer_kernel, n_ep, n_tp, pad_slot, chunks, taps - 1),
        out_shape=[
            jax.ShapeDtypeStruct((part, width), BF16),
            jax.ShapeDtypeStruct((tok, width), BF16),
            jax.ShapeDtypeStruct((tok, tok), BF16),
        ],
        in_specs=[hbm] * 13,
        out_specs=[hbm] * 3,
        scratch_shapes=[
            vm((rows_a, lanes), BF16),
            vm((HALO + rows_a, lanes), BF16),
            vm((HALO + rows_a, lanes), BF16),
            vm((taps, lanes), F32),
            vm((1, lanes), F32),
            vm((channels, width), BF16),
            vm((tok, width), BF16),
            vm((1, width), F32),
            vm((2, tok), jnp.int32),
            vm((2, tok), F32),
            vm((width, hid), BF16),
            vm((width, hid), BF16),
            vm((hid, width), BF16),
            vm((rows_a, lanes), BF16),
            vm((part, lanes), F32),
            vm((tok, width), BF16),
            vm((tok, tok), BF16),
            vm((tok, width + meta), BF16),
            vm((n_ep, rows, width + meta), BF16),
            vm((n_ep, slots, width), BF16),
            vm((total, width), BF16),
            vm((total // chunks, hid), BF16),
            vm((n_ep, slots, width), BF16),
            vm((n_ep, rows, width), BF16),
            vm((tok, width), BF16),
            vm((part, channels), BF16),
            vm((part, width), BF16),
            dma((13,)),
            dma((2 + n_ep,)),
            dma((2,)),
            dma((2,)),
            dma((n_tp,)),
            dma((n_tp,)),
            dma((n_ep,)),
            dma((n_ep,)),
            dma((n_ep, n_tp)),
            dma((n_ep, n_tp)),
            dma((n_ep, n_tp)),
            dma((n_ep, n_tp)),
            dma((n_ep,)),
            dma((n_ep,)),
        ],
        compiler_params=pltpu.CompilerParams(
            collective_id=0, has_side_effects=True, vmem_limit_bytes=60 * 1024 * 1024
        ),
        cost_estimate=pl.CostEstimate(
            flops=6 * total * width * hid, bytes_accessed=8 * width * hid, transcendentals=0
        ),
    )(
        out_gate, in_gate, conv_input, conv_taps, group_gain.reshape(1, lanes), mix_out_w,
        moe_in, moe_gain.reshape(1, width), route_ids.T, route_weight.T, gate_w, up_w, down_w,
    )


def finish_kernel(mixed_in, fin, place, mixed, out):
    mixed[...] = mixed_in[...]
    out[...] = tdot(place[...], fin[...]).astype(BF16)


def shards(*args):
    mixed, fin, place = layer(*args)
    tok, width = fin.shape
    block = 512
    cols = lambda rows: pl.BlockSpec((rows, block), lambda i: (0, i))
    return pl.pallas_call(
        finish_kernel,
        grid=(width // block,),
        out_shape=[
            jax.ShapeDtypeStruct(mixed.shape, BF16),
            jax.ShapeDtypeStruct((tok, width), BF16),
        ],
        in_specs=[cols(mixed.shape[0]), cols(tok), pl.BlockSpec((tok, tok), lambda i: (0, 0))],
        out_specs=[cols(mixed.shape[0]), cols(tok)],
        cost_estimate=pl.CostEstimate(
            flops=2 * tok * tok * width, bytes_accessed=8 * tok * width, transcendentals=0
        ),
    )(mixed, fin, place)


def solution(mesh):
    in_specs = (
        P("ep", "tp"),
        P("ep", "tp"),
        P("ep", "tp"),
        P(None, "tp"),
        P("tp"),
        P(),
        P(("ep", "tp"), None),
        P(),
        P(("ep", "tp"), None),
        P(("ep", "tp"), None),
        P(("ep", "tp"), None, None),
        P(("ep", "tp"), None, None),
        P(("ep", "tp"), None, None),
    )
    out_specs = (P(("ep", "tp"), None), P(("ep", "tp"), None))
    return jax.shard_map(shards, mesh=mesh, in_specs=in_specs, out_specs=out_specs, check_vma=False)
```

```python
import functools

import jax
import jax.numpy as jnp
from jax import lax
from jax.experimental import pallas as pl
from jax.experimental.pallas import tpu as pltpu
from jax.sharding import PartitionSpec as P

GROUP_CH = 64
HALO = 16
MESH = pl.DeviceIdType.MESH
BF16 = jnp.bfloat16
F32 = jnp.float32


def round_up(value, to):
    return (value + to - 1) // to * to


def tdot(a, b):
    return lax.dot_general(a, b, (((0,), (0,)), ((), ())), preferred_element_type=F32)


def dot_t(a, b):
    return lax.dot_general(a, b, (((1,), (1,)), ((), ())), preferred_element_type=F32)


def flip(index, mask):
    bit = 1
    out = index
    while bit <= mask:
        if mask & bit:
            out = out + bit * (1 - 2 * ((index // bit) % 2))
        bit *= 2
    return out


def layer_kernel(
    n_ep, n_tp, pad_slot, chunks, reach,
    og_hbm, ig_hbm, ci_hbm, taps_hbm, ggain_hbm, wm_hbm,
    x_hbm, mgain_hbm, ids_hbm, rw_hbm, wg_hbm, wu_hbm, wd_hbm,
    mixed_hbm, fin_hbm, place_hbm,
    og, ig, ci, taps, ggain, wm, x, mgain, ids, rw, wg, wu, wd,
    normed, gated, norm, place, sorted_rows, landed, picked, xin, hidden, comb, sums, fin, mixin, mixed,
    in_sem, out_sem, h_send, h_recv, m_send, m_recv, d_send, d_recv, p_send, p_recv, r_send, r_recv, f_send, f_recv,
):
    me_e = lax.axis_index("ep")
    me_t = lax.axis_index("tp")
    tok, width = x.shape
    rows = tok // n_ep
    slots = n_tp * pad_slot
    experts = n_ep * n_tp
    rows_a, lanes = og.shape
    part = rows_a // n_tp

    barrier = pltpu.get_barrier_semaphore()
    for k in range(1, n_ep):
        pl.semaphore_signal(
            barrier, inc=1, device_id={"ep": flip(me_e, k), "tp": me_t}, device_id_type=MESH
        )
    for j in range(1, n_tp):
        pl.semaphore_signal(
            barrier, inc=1, device_id={"ep": me_e, "tp": flip(me_t, j)}, device_id_type=MESH
        )
    nxt = lax.rem(me_e + 1, n_ep)
    own = pl.ds(HALO, rows_a)
    loads = {}
    for i, (name, src, dst) in enumerate((
        ("ids", ids_hbm, ids), ("rw", rw_hbm, rw), ("mgain", mgain_hbm, mgain), ("x", x_hbm, x),
        ("ig", ig_hbm, ig.at[own]), ("ci", ci_hbm, ci.at[own]), ("og", og_hbm, og),
        ("taps", taps_hbm, taps), ("ggain", ggain_hbm, ggain),
        ("wg", wg_hbm.at[0], wg), ("wu", wu_hbm.at[0], wu), ("wd", wd_hbm.at[0], wd), ("wm", wm_hbm, wm),
    )):
        loads[name] = pltpu.make_async_copy(src, dst, in_sem.at[i])
        loads[name].start()

    loads["ids"].wait()
    loads["rw"].wait()
    ids0, ids1 = ids[0:1, :], ids[1:2, :]
    sub_e = lax.broadcasted_iota(jnp.int32, (experts, tok), 0)
    hit0 = (ids0 == sub_e).astype(F32)
    hit1 = (ids1 == sub_e).astype(F32)
    both = (hit0 + hit1).astype(BF16)
    upper = (
        lax.broadcasted_iota(jnp.int32, (tok, tok), 0) < lax.broadcasted_iota(jnp.int32, (tok, tok), 1)
    ).astype(BF16)
    before = jnp.dot(both, upper, preferred_element_type=F32)
    rank0 = jnp.sum(before * hit0, axis=0, keepdims=True).astype(jnp.int32)
    rank1 = jnp.sum(before * hit1, axis=0, keepdims=True).astype(jnp.int32)
    group = ids0 // n_tp
    in_group = (group == (sub_e // n_tp)).astype(F32)
    rank_g = jnp.sum(before * in_group, axis=0, keepdims=True).astype(jnp.int32) // 2
    place[...] = (
        (group * rows + rank_g) == lax.broadcasted_iota(jnp.int32, (tok, tok), 0)
    ).astype(BF16)
    place_out = pltpu.make_async_copy(place, place_hbm, out_sem.at[0])
    place_out.start()
    cell0 = (ids0 - group * n_tp) * pad_slot + rank0
    cell1 = (ids1 - group * n_tp) * pad_slot + rank1
    sub_s = lax.broadcasted_iota(jnp.int32, (slots, tok), 0)
    weight = jnp.where(cell0 == sub_s, rw[0:1, :], 0.0) + jnp.where(cell1 == sub_s, rw[1:2, :], 0.0)
    high = weight.astype(BF16)
    low = (weight - high.astype(F32)).astype(BF16)
    cells = jnp.concatenate([high, low], axis=0)
    sorted_rows[:, width:] = dot_t(place[...], cells).astype(BF16)

    loads["mgain"].wait()
    loads["x"].wait()
    step = 32

    @pl.loop(0, tok // step)
    def _(i):
        at = pl.ds(pl.multiple_of(i * step, step), step)
        wide = x[at, :].astype(F32)
        scale = lax.rsqrt(jnp.mean(wide * wide, axis=-1, keepdims=True) + 1e-06)
        norm[at, :] = (wide * scale * mgain[...]).astype(BF16)

    @pl.loop(0, width // 512)
    def _(f):
        cols = pl.ds(pl.multiple_of(f * 512, 512), 512)
        sorted_rows[:, cols] = jnp.dot(
            place[...], norm[:, cols], preferred_element_type=F32
        ).astype(BF16)

    pl.semaphore_wait(barrier, n_ep - 1 + n_tp - 1)

    sends = []

    def send(src, dst, s_sem, r_sem, ep, tp):
        copy = pltpu.make_async_remote_copy(
            src_ref=src, dst_ref=dst, send_sem=s_sem, recv_sem=r_sem,
            device_id={"ep": ep, "tp": tp}, device_id_type=MESH,
        )
        copy.start()
        sends.append(copy)
        return copy

    loads["ig"].wait()
    loads["ci"].wait()
    tail, head = pl.ds(rows_a, HALO), pl.ds(0, HALO)
    halos = [
        send(ref.at[tail], ref.at[head], h_send.at[i], h_recv.at[i], nxt, me_t)
        for i, ref in enumerate((ig, ci))
    ]
    dispatch = {}
    for k in range(1, n_ep):
        to = flip(me_e, k)
        dispatch[k] = send(
            sorted_rows.at[pl.ds(pl.multiple_of(to * rows, rows), rows)],
            landed.at[k], d_send.at[k], d_recv.at[k], to, me_t,
        )
    landed[0] = sorted_rows[pl.ds(pl.multiple_of(me_e * rows, rows), rows), :]

    spread = {}

    def scatter(k):
        if k:
            dispatch[k].wait_recv()
        chosen = (landed[k, :, pl.ds(width, slots)].astype(F32) != 0.0).astype(BF16)
        picked[k] = tdot(chosen, landed[k, :, 0:width]).astype(BF16)
        for j in range(n_tp - 1, 0, -1):
            to = flip(me_t, j)
            spread[k, j] = send(
                picked.at[k, pl.ds(pl.multiple_of(to * pad_slot, pad_slot), pad_slot)],
                xin.at[pl.ds((k * n_tp + j) * pad_slot, pad_slot)],
                p_send.at[k, j], p_recv.at[k, j], me_e, to,
            )
        xin[pl.ds(k * n_tp * pad_slot, pad_slot), :] = picked[
            k, pl.ds(pl.multiple_of(me_t * pad_slot, pad_slot), pad_slot), :
        ]

    scatter(0)

    loads["og"].wait()
    loads["taps"].wait()
    loads["ggain"].wait()
    for copy in halos:
        copy.wait_recv()

    @pl.when(me_e == 0)
    def _():
        ig[0:HALO, :] = jnp.zeros((HALO, lanes), BF16)

    same = (
        lax.broadcasted_iota(jnp.int32, (lanes, lanes), 0) // GROUP_CH
        == lax.broadcasted_iota(jnp.int32, (lanes, lanes), 1) // GROUP_CH
    ).astype(BF16)
    own_lanes = pl.ds(pl.multiple_of(me_t * lanes, lanes), lanes)
    mixes = []
    for j in range(n_tp - 1, -1, -1):
        to = flip(me_t, j)
        base = pl.multiple_of(to * part, part)
        cstep = 64

        @pl.loop(0, part // cstep)
        def _(i):
            at = pl.multiple_of(base + i * cstep, cstep)
            span = pl.ds(at, cstep + HALO)
            product = ig[span, :].astype(F32) * ci[span, :].astype(F32)
            total = taps[reach : reach + 1, :] * product[HALO:, :]
            for back_by in range(1, reach + 1):
                total = total + taps[reach - back_by : reach - back_by + 1, :] * (
                    product[HALO - back_by : HALO - back_by + cstep, :]
                )
            gated[pl.ds(pl.multiple_of(i * cstep, cstep), cstep), :] = (
                og[pl.ds(at, cstep), :].astype(F32) * total
            )

        value = gated[...]
        square = value * value
        s_high = square.astype(BF16)
        s_low = (square - s_high.astype(F32)).astype(BF16)
        mean = (
            jnp.dot(s_high, same, preferred_element_type=F32)
            + jnp.dot(s_low, same, preferred_element_type=F32)
        ) * (1.0 / GROUP_CH)
        done = (value * lax.rsqrt(mean + 1e-06) * ggain[...]).astype(BF16)
        if j:
            normed[pl.ds(base, part), :] = done
            mixes.append(send(
                normed.at[pl.ds(base, part)], mixin.at[:, own_lanes],
                m_send.at[j], m_recv.at[j], me_e, to,
            ))
        else:
            mixin[:, own_lanes] = done

    hid = wg.shape[1]
    per = n_ep // chunks
    many = per * slots
    back = {}
    mine = pl.ds(pl.multiple_of(me_t * pad_slot, pad_slot), pad_slot)
    here = pl.ds(pl.multiple_of(me_e * rows, rows), rows)

    def expert(c):
        for k in range(c * per, (c + 1) * per):
            for j in range(1, n_tp):
                spread[k, j].wait_recv()
        span = pl.ds(c * many, many)

        @pl.loop(0, hid // 256)
        def _(f):
            cols = pl.ds(pl.multiple_of(f * 256, 256), 256)
            gate = jnp.dot(xin[span, :], wg[:, cols], preferred_element_type=F32)
            up = jnp.dot(xin[span, :], wu[:, cols], preferred_element_type=F32)
            hidden[:, cols] = (gate / (1.0 + jnp.exp(-gate)) * up).astype(BF16)

        @pl.loop(0, width // 512)
        def _(f):
            cols = pl.ds(pl.multiple_of(f * 512, 512), 512)
            xin[span, cols] = jnp.dot(
                hidden[...], wd[:, cols], preferred_element_type=F32
            ).astype(BF16)

    def give_back(c):
        for k in range(c * per, (c + 1) * per):
            for j in range(n_tp - 1, 0, -1):
                back[k, j] = send(
                    xin.at[pl.ds((k * n_tp + j) * pad_slot, pad_slot)],
                    comb.at[k, mine], r_send.at[k, j], r_recv.at[k, j], me_e, flip(me_t, j),
                )
            comb[k, mine, :] = xin[pl.ds(k * slots, pad_slot), :]

    home = {}

    def combine(k):
        for j in range(1, n_tp):
            back[k, j].wait_recv()
        total = jnp.dot(
            landed[k, :, pl.ds(width, slots)], comb[k], preferred_element_type=F32
        ) + jnp.dot(
            landed[k, :, pl.ds(width + slots, slots)], comb[k], preferred_element_type=F32
        )
        if k == 0:
            fin[here, :] = total.astype(BF16)
            return
        sums[k] = total.astype(BF16)
        home[k] = send(sums.at[k], fin.at[here], f_send.at[k], f_recv.at[k], flip(me_e, k), me_t)

    half = n_ep // 2
    near = list(range(chunks // 2))
    far = list(range(chunks // 2, chunks))
    for k in range(1, half):
        scatter(k)
    for name in ("wg", "wu", "wd", "wm"):
        loads[name].wait()
    expert(near[0])
    scatter(half)
    for c in near[1:]:
        expert(c)
    scatter(half + 1)
    for copy in mixes:
        copy.wait_recv()

    @pl.loop(0, width // 512)
    def _(f):
        cols = pl.ds(pl.multiple_of(f * 512, 512), 512)
        mixed[:, cols] = jnp.dot(mixin[...], wm[:, cols], preferred_element_type=F32).astype(BF16)

    mixed_out = pltpu.make_async_copy(mixed, mixed_hbm, out_sem.at[1])
    mixed_out.start()
    for k in range(half + 2, n_ep):
        scatter(k)
    for c in far:
        expert(c)
        give_back(c)
    for c in near[::-1]:
        give_back(c)
    order = [k for c in far + near[::-1] for k in range(c * per, (c + 1) * per)]
    for k in order:
        combine(k)
    fin_out = []

    def finish(k):
        block = pl.ds(pl.multiple_of(flip(me_e, k) * rows, rows), rows)
        copy = pltpu.make_async_copy(fin.at[block], fin_hbm.at[block], out_sem.at[2 + k])
        copy.start()
        fin_out.append(copy)

    for k in order:
        if k:
            home[k].wait_recv()
        finish(k)
    for copy in sends:
        copy.wait_send()
    for copy in [place_out, mixed_out] + fin_out:
        copy.wait()


def layer(
    out_gate, in_gate, conv_input, conv_taps, group_gain, mix_out_w,
    moe_in, moe_gain, route_ids, route_weight, gate_w, up_w, down_w,
):
    n_ep, n_tp = lax.axis_size("ep"), lax.axis_size("tp")
    tok, width = moe_in.shape
    hid = gate_w.shape[2]
    pad_slot = round_up(2 * tok // (n_ep * n_tp), 16)
    rows = tok // n_ep
    slots = n_tp * pad_slot
    meta = round_up(2 * slots, 128)
    total = n_ep * slots
    chunks = 4
    rows_a, lanes = out_gate.shape
    part = rows_a // n_tp
    channels = mix_out_w.shape[0]
    taps = conv_taps.shape[0]
    hbm = pl.BlockSpec(memory_space=pl.ANY)
    dma = pltpu.SemaphoreType.DMA
    vm = pltpu.VMEM
    return pl.pallas_call(
        functools.partial(layer_kernel, n_ep, n_tp, pad_slot, chunks, taps - 1),
        out_shape=[
            jax.ShapeDtypeStruct((part, width), BF16),
            jax.ShapeDtypeStruct((tok, width), BF16),
            jax.ShapeDtypeStruct((tok, tok), BF16),
        ],
        in_specs=[hbm] * 13,
        out_specs=[hbm] * 3,
        scratch_shapes=[
            vm((rows_a, lanes), BF16),
            vm((HALO + rows_a, lanes), BF16),
            vm((HALO + rows_a, lanes), BF16),
            vm((taps, lanes), F32),
            vm((1, lanes), F32),
            vm((channels, width), BF16),
            vm((tok, width), BF16),
            vm((1, width), F32),
            vm((2, tok), jnp.int32),
            vm((2, tok), F32),
            vm((width, hid), BF16),
            vm((width, hid), BF16),
            vm((hid, width), BF16),
            vm((rows_a, lanes), BF16),
            vm((part, lanes), F32),
            vm((tok, width), BF16),
            vm((tok, tok), BF16),
            vm((tok, width + meta), BF16),
            vm((n_ep, rows, width + meta), BF16),
            vm((n_ep, slots, width), BF16),
            vm((total, width), BF16),
            vm((total // chunks, hid), BF16),
            vm((n_ep, slots, width), BF16),
            vm((n_ep, rows, width), BF16),
            vm((tok, width), BF16),
            vm((part, channels), BF16),
            vm((part, width), BF16),
            dma((13,)),
            dma((2 + n_ep,)),
            dma((2,)),
            dma((2,)),
            dma((n_tp,)),
            dma((n_tp,)),
            dma((n_ep,)),
            dma((n_ep,)),
            dma((n_ep, n_tp)),
            dma((n_ep, n_tp)),
            dma((n_ep, n_tp)),
            dma((n_ep, n_tp)),
            dma((n_ep,)),
            dma((n_ep,)),
        ],
        compiler_params=pltpu.CompilerParams(
            collective_id=0, has_side_effects=True, vmem_limit_bytes=60 * 1024 * 1024
        ),
        cost_estimate=pl.CostEstimate(
            flops=6 * total * width * hid, bytes_accessed=8 * width * hid, transcendentals=0
        ),
    )(
        out_gate, in_gate, conv_input, conv_taps, group_gain.reshape(1, lanes), mix_out_w,
        moe_in, moe_gain.reshape(1, width), route_ids.T, route_weight.T, gate_w, up_w, down_w,
    )


def finish_kernel(mixed_in, fin, place, mixed, out):
    mixed[...] = mixed_in[...]
    out[...] = tdot(place[...], fin[...]).astype(BF16)


def shards(*args):
    mixed, fin, place = layer(*args)
    tok, width = fin.shape
    block = 512
    cols = lambda rows: pl.BlockSpec((rows, block), lambda i: (0, i))
    return pl.pallas_call(
        finish_kernel,
        grid=(width // block,),
        out_shape=[
            jax.ShapeDtypeStruct(mixed.shape, BF16),
            jax.ShapeDtypeStruct((tok, width), BF16),
        ],
        in_specs=[cols(mixed.shape[0]), cols(tok), pl.BlockSpec((tok, tok), lambda i: (0, 0))],
        out_specs=[cols(mixed.shape[0]), cols(tok)],
        cost_estimate=pl.CostEstimate(
            flops=2 * tok * tok * width, bytes_accessed=8 * tok * width, transcendentals=0
        ),
    )(mixed, fin, place)


def solution(mesh):
    in_specs = (
        P("ep", "tp"),
        P("ep", "tp"),
        P("ep", "tp"),
        P(None, "tp"),
        P("tp"),
        P(),
        P(("ep", "tp"), None),
        P(),
        P(("ep", "tp"), None),
        P(("ep", "tp"), None),
        P(("ep", "tp"), None, None),
        P(("ep", "tp"), None, None),
        P(("ep", "tp"), None, None),
    )
    out_specs = (P(("ep", "tp"), None), P(("ep", "tp"), None))
    return jax.shard_map(shards, mesh=mesh, in_specs=in_specs, out_specs=out_specs, check_vma=False)
```

```python
import functools
import math

import jax
import jax.numpy as jnp
from jax import lax
from jax.experimental import pallas as pl
from jax.experimental.pallas import tpu as pltpu
from jax.sharding import PartitionSpec as P

GROUP_CH = 64
HALO = 16
VMEM_BYTES = 60 * 1024 * 1024
SPARE = 6 << 20
MESH = pl.DeviceIdType.MESH
BF16 = jnp.bfloat16
F32 = jnp.float32


def round_up(value, to):
    return (value + to - 1) // to * to


def tdot(a, b):
    return lax.dot_general(a, b, (((0,), (0,)), ((), ())), preferred_element_type=F32)


def dot_t(a, b):
    return lax.dot_general(a, b, (((1,), (1,)), ((), ())), preferred_element_type=F32)


def flip(index, mask):
    bit = 1
    out = index
    while bit <= mask:
        if mask & bit:
            out = out + bit * (1 - 2 * ((index // bit) % 2))
        bit *= 2
    return out


def layer_kernel(
    n_ep, n_tp, pad_slot, reach,
    og_hbm, ig_hbm, ci_hbm, taps_hbm, ggain_hbm, wm_hbm,
    x_hbm, mgain_hbm, ids_hbm, rw_hbm, wg_hbm, wu_hbm, wd_hbm,
    mixed, fin, place,
    og, ig, ci, taps, ggain, wm, x, mgain, ids, rw, wg, wu, wd,
    normed, gated, norm, sorted_rows, landed, picked, xin, hidden, comb, sums, mixin,
    in_sem, h_send, h_recv, m_send, m_recv, d_send, d_recv, p_send, p_recv, r_send, r_recv, f_send, f_recv,
):
    me_e = lax.axis_index("ep")
    me_t = lax.axis_index("tp")
    tok, width = x.shape
    rows = tok // n_ep
    slots = n_tp * pad_slot
    experts = n_ep * n_tp
    rows_a, lanes = og.shape
    part = rows_a // n_tp
    quarter = n_ep // 4

    barrier = pltpu.get_barrier_semaphore()
    for k in range(1, n_ep):
        pl.semaphore_signal(
            barrier, inc=1, device_id={"ep": flip(me_e, k), "tp": me_t}, device_id_type=MESH
        )
    for j in range(1, n_tp):
        pl.semaphore_signal(
            barrier, inc=1, device_id={"ep": me_e, "tp": flip(me_t, j)}, device_id_type=MESH
        )
    nxt = lax.rem(me_e + 1, n_ep)
    own = pl.ds(HALO, rows_a)
    loads = {}
    for i, (name, src, dst) in enumerate((
        ("ids", ids_hbm, ids), ("rw", rw_hbm, rw), ("mgain", mgain_hbm, mgain), ("x", x_hbm, x),
        ("ig", ig_hbm, ig.at[own]), ("ci", ci_hbm, ci.at[own]), ("og", og_hbm, og),
        ("taps", taps_hbm, taps), ("ggain", ggain_hbm, ggain),
        ("wg", wg_hbm.at[0], wg), ("wu", wu_hbm.at[0], wu), ("wd", wd_hbm.at[0], wd), ("wm", wm_hbm, wm),
    )):
        loads[name] = pltpu.make_async_copy(src, dst, in_sem.at[i])
        loads[name].start()

    loads["ids"].wait()
    loads["rw"].wait()
    ids0, ids1 = ids[0:1, :], ids[1:2, :]
    sub_e = lax.broadcasted_iota(jnp.int32, (experts, tok), 0)
    hit0 = (ids0 == sub_e).astype(F32)
    hit1 = (ids1 == sub_e).astype(F32)
    both = (hit0 + hit1).astype(BF16)
    upper = (
        lax.broadcasted_iota(jnp.int32, (tok, tok), 0) < lax.broadcasted_iota(jnp.int32, (tok, tok), 1)
    ).astype(BF16)
    before = jnp.dot(both, upper, preferred_element_type=F32)
    rank0 = jnp.sum(before * hit0, axis=0, keepdims=True).astype(jnp.int32)
    rank1 = jnp.sum(before * hit1, axis=0, keepdims=True).astype(jnp.int32)
    group = ids0 // n_tp
    in_group = (group == (sub_e // n_tp)).astype(F32)
    rank_g = jnp.sum(before * in_group, axis=0, keepdims=True).astype(jnp.int32) // 2
    place[...] = (
        (group * rows + rank_g) == lax.broadcasted_iota(jnp.int32, (tok, tok), 0)
    ).astype(BF16)
    cell0 = (ids0 - group * n_tp) * pad_slot + rank0
    cell1 = (ids1 - group * n_tp) * pad_slot + rank1
    sub_s = lax.broadcasted_iota(jnp.int32, (slots, tok), 0)
    weight = jnp.where(cell0 == sub_s, rw[0:1, :], 0.0) + jnp.where(cell1 == sub_s, rw[1:2, :], 0.0)
    high = weight.astype(BF16)
    low = (weight - high.astype(F32)).astype(BF16)
    cells = jnp.concatenate([high, low], axis=0)
    sorted_rows[:, width:] = dot_t(place[...], cells).astype(BF16)

    loads["mgain"].wait()
    loads["x"].wait()
    step = 32

    @pl.loop(0, tok // step)
    def _(i):
        at = pl.ds(pl.multiple_of(i * step, step), step)
        wide = x[at, :].astype(F32)
        scale = lax.rsqrt(jnp.mean(wide * wide, axis=-1, keepdims=True) + 1e-06)
        norm[at, :] = (wide * scale * mgain[...]).astype(BF16)

    @pl.loop(0, width // 512)
    def _(f):
        cols = pl.ds(pl.multiple_of(f * 512, 512), 512)
        sorted_rows[:, cols] = jnp.dot(
            place[...], norm[:, cols], preferred_element_type=F32
        ).astype(BF16)

    pl.semaphore_wait(barrier, n_ep - 1 + n_tp - 1)

    others = pl.ds(0, (n_tp - 1) * pad_slot)

    def settle(sem, like):
        pltpu.make_async_copy(like, like, sem).wait()

    def send(src, dst, s_sem, r_sem, ep, tp):
        copy = pltpu.make_async_remote_copy(
            src_ref=src, dst_ref=dst, send_sem=s_sem, recv_sem=r_sem,
            device_id={"ep": ep, "tp": tp}, device_id_type=MESH,
        )
        copy.start()
        return copy

    loads["ig"].wait()
    loads["ci"].wait()
    tail, head = pl.ds(rows_a, HALO), pl.ds(0, HALO)
    halos = [
        pltpu.make_async_remote_copy(
            src_ref=ref.at[tail], dst_ref=ref.at[head], send_sem=h_send, recv_sem=h_recv,
            device_id={"ep": nxt, "tp": me_t}, device_id_type=MESH,
        )
        for ref in (ig, ci)
    ]

    @pl.when(me_e < n_ep - 1)
    def _():
        for copy in halos:
            copy.start()

    dispatch = {}
    for k in range(1, n_ep):
        to = flip(me_e, k)
        dispatch[k] = send(
            sorted_rows.at[pl.ds(pl.multiple_of(to * rows, rows), rows)],
            landed.at[k], d_send, d_recv.at[k], to, me_t,
        )
    landed[0] = sorted_rows[pl.ds(pl.multiple_of(me_e * rows, rows), rows), :]

    def scatter(k):
        if k:
            dispatch[k].wait_recv()
        chosen = (landed[k, :, pl.ds(width, slots)].astype(F32) != 0.0).astype(BF16)
        picked[k] = tdot(chosen, landed[k, :, 0:width]).astype(BF16)
        for j in range(n_tp - 1, 0, -1):
            to = flip(me_t, j)
            send(
                picked.at[k, pl.ds(pl.multiple_of(to * pad_slot, pad_slot), pad_slot)],
                xin.at[pl.ds((k * n_tp + j) * pad_slot, pad_slot)],
                p_send, p_recv.at[k // quarter], me_e, to,
            )
        xin[pl.ds(k * n_tp * pad_slot, pad_slot), :] = picked[
            k, pl.ds(pl.multiple_of(me_t * pad_slot, pad_slot), pad_slot), :
        ]

    own_lanes = pl.ds(pl.multiple_of(me_t * lanes, lanes), lanes)

    def conv_ready():
        for name in ("og", "taps", "ggain"):
            loads[name].wait()

        @pl.when(me_e > 0)
        def _():
            settle(h_recv, ig.at[pl.ds(0, 2 * HALO)])

        @pl.when(me_e == 0)
        def _():
            ig[0:HALO, :] = jnp.zeros((HALO, lanes), BF16)

    def conv(j):
        same = (
            lax.broadcasted_iota(jnp.int32, (lanes, lanes), 0) // GROUP_CH
            == lax.broadcasted_iota(jnp.int32, (lanes, lanes), 1) // GROUP_CH
        ).astype(BF16)
        base = pl.multiple_of(flip(me_t, j) * part, part)
        cstep = 64

        @pl.loop(0, part // cstep)
        def _(i):
            at = pl.multiple_of(base + i * cstep, cstep)
            span = pl.ds(at, cstep + HALO)
            product = ig[span, :].astype(F32) * ci[span, :].astype(F32)
            total = taps[reach : reach + 1, :] * product[HALO:, :]
            for back_by in range(1, reach + 1):
                total = total + taps[reach - back_by : reach - back_by + 1, :] * (
                    product[HALO - back_by : HALO - back_by + cstep, :]
                )
            gated[pl.ds(pl.multiple_of(i * cstep, cstep), cstep), :] = (
                og[pl.ds(at, cstep), :].astype(F32) * total
            )

        value = gated[...]
        square = value * value
        s_high = square.astype(BF16)
        s_low = (square - s_high.astype(F32)).astype(BF16)
        mean = (
            jnp.dot(s_high, same, preferred_element_type=F32)
            + jnp.dot(s_low, same, preferred_element_type=F32)
        ) * (1.0 / GROUP_CH)
        done = (value * lax.rsqrt(mean + 1e-06) * ggain[...]).astype(BF16)
        if j:
            normed[pl.ds(base, part), :] = done
        else:
            mixin[:, own_lanes] = done

    def mix_send(j):
        to = flip(me_t, j)
        send(
            normed.at[pl.ds(pl.multiple_of(to * part, part), part)], mixin.at[:, own_lanes],
            m_send, m_recv, me_e, to,
        )

    def mixer():
        settle(m_recv, mixin.at[:, pl.ds(0, (n_tp - 1) * lanes)])

        @pl.loop(0, width // 512)
        def _(f):
            cols = pl.ds(pl.multiple_of(f * 512, 512), 512)
            mixed[:, cols] = jnp.dot(mixin[...], wm[:, cols], preferred_element_type=F32).astype(BF16)

    hid = wg.shape[1]
    mine = pl.ds(pl.multiple_of(me_t * pad_slot, pad_slot), pad_slot)
    here = pl.ds(pl.multiple_of(me_e * rows, rows), rows)

    def expert(first, count):
        settle(p_recv.at[first // quarter], xin.at[pl.ds(first * slots, count * (n_tp - 1) * pad_slot)])
        span = pl.ds(first * slots, count * slots)
        hid_rows = pl.ds(0, count * slots)

        @pl.loop(0, hid // 256)
        def _(f):
            cols = pl.ds(pl.multiple_of(f * 256, 256), 256)
            gate = jnp.dot(xin[span, :], wg[:, cols], preferred_element_type=F32)
            up = jnp.dot(xin[span, :], wu[:, cols], preferred_element_type=F32)
            hidden[hid_rows, cols] = (gate / (1.0 + jnp.exp(-gate)) * up).astype(BF16)

        @pl.loop(0, width // 512)
        def _(f):
            cols = pl.ds(pl.multiple_of(f * 512, 512), 512)
            xin[span, cols] = jnp.dot(
                hidden[hid_rows, :], wd[:, cols], preferred_element_type=F32
            ).astype(BF16)

    def give_back(first, count):
        for k in range(first, first + count):
            for j in range(n_tp - 1, 0, -1):
                send(
                    xin.at[pl.ds((k * n_tp + j) * pad_slot, pad_slot)],
                    comb.at[k, mine], r_send, r_recv.at[k], me_e, flip(me_t, j),
                )
            comb[k, mine, :] = xin[pl.ds(k * slots, pad_slot), :]


    def combine(k):
        settle(r_recv.at[k], comb.at[k, others])
        total = jnp.dot(
            landed[k, :, pl.ds(width, slots)], comb[k], preferred_element_type=F32
        ) + jnp.dot(
            landed[k, :, pl.ds(width + slots, slots)], comb[k], preferred_element_type=F32
        )
        if k == 0:
            fin[here, :] = total.astype(BF16)
            return
        sums[k] = total.astype(BF16)
        send(sums.at[k], fin.at[here], f_send, f_recv, flip(me_e, k), me_t)

    half = n_ep // 2
    scatter(0)
    conv_ready()
    for j in range(n_tp - 1, 0, -1):
        conv(j)
        mix_send(j)
    conv(0)
    for k in range(1, half):
        scatter(k)
    loads["wm"].wait()
    mixer()
    for name in ("wg", "wu", "wd"):
        loads[name].wait()
    for k in range(half, half + quarter):
        scatter(k)
    expert(0, quarter)
    for k in range(half + quarter, n_ep):
        scatter(k)
    expert(half, quarter)
    give_back(half, quarter)
    expert(half + quarter, quarter)
    give_back(half + quarter, quarter)
    for k in range(half, half + quarter):
        combine(k)
    expert(quarter, quarter)
    give_back(quarter, quarter)
    give_back(0, quarter)
    for k in range(half + quarter, n_ep):
        combine(k)
    for k in range(half - 1, quarter - 1, -1):
        combine(k)
    for k in range(quarter - 1, -1, -1):
        combine(k)
    settle(f_recv, fin.at[pl.ds(0, (n_ep - 1) * rows)])
    @pl.when(me_e < n_ep - 1)
    def _():
        settle(h_send, ig.at[pl.ds(0, 2 * HALO)])

    settle(d_send, sorted_rows.at[pl.ds(0, (n_ep - 1) * rows)])
    settle(m_send, normed.at[pl.ds(0, (n_tp - 1) * part)])
    settle(p_send, picked.at[:, others])
    settle(r_send, comb.at[:, others])
    settle(f_send, sums.at[pl.ds(0, n_ep - 1)])


def layer(
    out_gate, in_gate, conv_input, conv_taps, group_gain, mix_out_w,
    moe_in, moe_gain, route_ids, route_weight, gate_w, up_w, down_w,
):
    n_ep, n_tp = lax.axis_size("ep"), lax.axis_size("tp")
    tok, width = moe_in.shape
    hid = gate_w.shape[2]
    pad_slot = round_up(2 * tok // (n_ep * n_tp), 16)
    rows = tok // n_ep
    slots = n_tp * pad_slot
    meta = round_up(2 * slots, 128)
    total = n_ep * slots
    rows_a, lanes = out_gate.shape
    part = rows_a // n_tp
    channels = mix_out_w.shape[0]
    taps = conv_taps.shape[0]
    hbm = pl.BlockSpec(memory_space=pltpu.HBM)
    dma = pltpu.SemaphoreType.DMA
    vm = pltpu.VMEM
    scratch = [
        vm((rows_a, lanes), BF16),
        vm((HALO + rows_a, lanes), BF16),
        vm((HALO + rows_a, lanes), BF16),
        vm((taps, lanes), F32),
        vm((1, lanes), F32),
        vm((channels, width), BF16),
        vm((tok, width), BF16),
        vm((1, width), F32),
        vm((2, tok), jnp.int32),
        vm((2, tok), F32),
        vm((width, hid), BF16),
        vm((width, hid), BF16),
        vm((hid, width), BF16),
        vm((rows_a, lanes), BF16),
        vm((part, lanes), F32),
        vm((tok, width), BF16),
        vm((tok, width + meta), BF16),
        vm((n_ep, rows, width + meta), BF16),
        vm((n_ep, slots, width), BF16),
        vm((total, width), BF16),
        vm((total // 4, hid), BF16),
        vm((n_ep, slots, width), BF16),
        vm((n_ep, rows, width), BF16),
        vm((part, channels), BF16),
        dma((13,)),
        dma(()),
        dma(()),
        dma(()),
        dma(()),
        dma(()),
        dma((n_ep,)),
        dma(()),
        dma((4,)),
        dma(()),
        dma((n_ep,)),
        dma(()),
        dma(()),
    ]
    held = 2 * (part * width + tok * width + tok * tok) + sum(
        math.prod(one.shape) * jnp.dtype(one.dtype).itemsize for one in scratch if one.memory_space == vm
    )
    return pl.pallas_call(
        functools.partial(layer_kernel, n_ep, n_tp, pad_slot, taps - 1),
        out_shape=[
            jax.ShapeDtypeStruct((part, width), BF16),
            jax.ShapeDtypeStruct((tok, width), BF16),
            jax.ShapeDtypeStruct((tok, tok), BF16),
        ],
        in_specs=[hbm] * 13,
        out_specs=[pl.BlockSpec(memory_space=vm)] * 3,
        scratch_shapes=scratch,
        compiler_params=pltpu.CompilerParams(
            collective_id=0, has_side_effects=True, vmem_limit_bytes=min(held + SPARE, VMEM_BYTES)
        ),
        cost_estimate=pl.CostEstimate(
            flops=6 * total * width * hid, bytes_accessed=8 * width * hid, transcendentals=0
        ),
    )(*[pltpu.with_memory_space_constraint(a, pltpu.HBM) for a in (
        out_gate, in_gate, conv_input, conv_taps, group_gain.reshape(1, lanes), mix_out_w,
        moe_in, moe_gain.reshape(1, width), route_ids.T, route_weight.T, gate_w, up_w, down_w,
    )])


def finish_kernel(mixed_in, fin, place, mixed, out, done, sem):
    copies = [pltpu.make_async_copy(mixed_in, mixed, sem.at[0])]
    copies[0].start()
    block = 512
    for i in range(done.shape[1] // block):
        cols = pl.ds(i * block, block)
        done[:, cols] = tdot(place[...], fin[:, cols]).astype(BF16)
        copies.append(pltpu.make_async_copy(done.at[:, cols], out.at[:, cols], sem.at[1 + i]))
        copies[-1].start()
    for copy in copies:
        copy.wait()


def shards(*args):
    mixed, fin, place = layer(*args)
    tok, width = fin.shape
    vm = pl.BlockSpec(memory_space=pltpu.VMEM)
    hbm = pl.BlockSpec(memory_space=pl.ANY)
    return pl.pallas_call(
        finish_kernel,
        out_shape=[
            jax.ShapeDtypeStruct(mixed.shape, BF16),
            jax.ShapeDtypeStruct((tok, width), BF16),
        ],
        in_specs=[vm, vm, vm],
        out_specs=[hbm, hbm],
        scratch_shapes=[pltpu.VMEM((tok, width), BF16), pltpu.SemaphoreType.DMA((1 + width // 512,))],
        compiler_params=pltpu.CompilerParams(vmem_limit_bytes=8 << 20),
        cost_estimate=pl.CostEstimate(
            flops=2 * tok * tok * width, bytes_accessed=8 * tok * width, transcendentals=0
        ),
    )(mixed, fin, place)


def solution(mesh):
    in_specs = (
        P("ep", "tp"),
        P("ep", "tp"),
        P("ep", "tp"),
        P(None, "tp"),
        P("tp"),
        P(),
        P(("ep", "tp"), None),
        P(),
        P(("ep", "tp"), None),
        P(("ep", "tp"), None),
        P(("ep", "tp"), None, None),
        P(("ep", "tp"), None, None),
        P(("ep", "tp"), None, None),
    )
    out_specs = (P(("ep", "tp"), None), P(("ep", "tp"), None))
    return jax.shard_map(shards, mesh=mesh, in_specs=in_specs, out_specs=out_specs, check_vma=False)
```

```python
import functools
import math

import jax
import jax.numpy as jnp
from jax import lax
from jax.experimental import pallas as pl
from jax.experimental.pallas import tpu as pltpu
from jax.sharding import PartitionSpec as P

GROUP_CH = 64
HALO = 16
VMEM_BYTES = 60 * 1024 * 1024
SPARE = 6 << 20
MESH = pl.DeviceIdType.MESH
BF16 = jnp.bfloat16
F32 = jnp.float32


def round_up(value, to):
    return (value + to - 1) // to * to


def tdot(a, b):
    return lax.dot_general(a, b, (((0,), (0,)), ((), ())), preferred_element_type=F32)


def dot_t(a, b):
    return lax.dot_general(a, b, (((1,), (1,)), ((), ())), preferred_element_type=F32)


def flip(index, mask):
    bit = 1
    out = index
    while bit <= mask:
        if mask & bit:
            out = out + bit * (1 - 2 * ((index // bit) % 2))
        bit *= 2
    return out


def layer_kernel(
    n_ep, n_tp, pad_slot, reach,
    og_hbm, ig_hbm, ci_hbm, taps_hbm, ggain_hbm, wm_hbm,
    x_hbm, mgain_hbm, ids_hbm, rw_hbm, wg_hbm, wu_hbm, wd_hbm,
    mixed, fin, place,
    og, ig, ci, taps, ggain, wm, x, mgain, ids, rw, wg, wu, wd,
    normed, gated, raw, sorted_rows, landed, picked, xin, hidden, comb, sums, mixin,
    in_sem, h_send, h_recv, m_send, m_recv, d_send, d_recv, p_send, p_recv, r_send, r_recv, f_send, f_recv,
):
    me_e = lax.axis_index("ep")
    me_t = lax.axis_index("tp")
    tok, width = x.shape
    rows = tok // n_ep
    slots = n_tp * pad_slot
    experts = n_ep * n_tp
    rows_a, lanes = og.shape
    part = rows_a // n_tp
    quarter = n_ep // 4
    q0, q1, q2, q3 = [list(range(i * quarter, (i + 1) * quarter)) for i in range(4)]

    middle = ((me_e // quarter + 1) // 2) % 2
    split = quarter // 2
    leaving = q1 + q0 + q2 + q3, q2 + q0 + q1 + q3
    coming = q0 + q2[:split] + q1 + q2[split:] + q3, q0 + q1 + q2 + q3

    def pick(orders, step, of=lambda k: k):
        outer, inner = orders[0][step], orders[1][step]
        if outer == inner:
            return of(outer)
        return middle * of(inner) + (1 - middle) * of(outer)

    def peer(k):
        return flip(me_e, k)

    barrier = pltpu.get_barrier_semaphore()
    for k in range(1, n_ep):
        pl.semaphore_signal(
            barrier, inc=1, device_id={"ep": flip(me_e, k), "tp": me_t}, device_id_type=MESH
        )
    for j in range(1, n_tp):
        pl.semaphore_signal(
            barrier, inc=1, device_id={"ep": me_e, "tp": flip(me_t, j)}, device_id_type=MESH
        )
    nxt = lax.rem(me_e + 1, n_ep)
    own = pl.ds(HALO, rows_a)
    loads = {}
    for i, (name, src, dst) in enumerate((
        ("ids", ids_hbm, ids), ("rw", rw_hbm, rw), ("mgain", mgain_hbm, mgain), ("x", x_hbm, x),
        ("ig", ig_hbm, ig.at[own]), ("ci", ci_hbm, ci.at[own]), ("og", og_hbm, og),
        ("taps", taps_hbm, taps), ("ggain", ggain_hbm, ggain),
        ("wg", wg_hbm.at[0], wg), ("wu", wu_hbm.at[0], wu), ("wd", wd_hbm.at[0], wd), ("wm", wm_hbm, wm),
    )):
        loads[name] = pltpu.make_async_copy(src, dst, in_sem.at[i])
        loads[name].start()

    loads["ids"].wait()
    loads["rw"].wait()
    ids0, ids1 = ids[0:1, :], ids[1:2, :]
    sub_e = lax.broadcasted_iota(jnp.int32, (experts, tok), 0)
    hit0 = (ids0 == sub_e).astype(F32)
    hit1 = (ids1 == sub_e).astype(F32)
    both = (hit0 + hit1).astype(BF16)
    upper = (
        lax.broadcasted_iota(jnp.int32, (tok, tok), 0) < lax.broadcasted_iota(jnp.int32, (tok, tok), 1)
    ).astype(BF16)
    before = jnp.dot(both, upper, preferred_element_type=F32)
    rank0 = jnp.sum(before * hit0, axis=0, keepdims=True).astype(jnp.int32)
    rank1 = jnp.sum(before * hit1, axis=0, keepdims=True).astype(jnp.int32)
    group = ids0 // n_tp
    in_group = (group == (sub_e // n_tp)).astype(F32)
    rank_g = jnp.sum(before * in_group, axis=0, keepdims=True).astype(jnp.int32) // 2
    place[...] = (
        (group * rows + rank_g) == lax.broadcasted_iota(jnp.int32, (tok, tok), 0)
    ).astype(BF16)
    cell0 = (ids0 - group * n_tp) * pad_slot + rank0
    cell1 = (ids1 - group * n_tp) * pad_slot + rank1
    sub_s = lax.broadcasted_iota(jnp.int32, (slots, tok), 0)
    weight = jnp.where(cell0 == sub_s, rw[0:1, :], 0.0) + jnp.where(cell1 == sub_s, rw[1:2, :], 0.0)
    high = weight.astype(BF16)
    low = (weight - high.astype(F32)).astype(BF16)
    cells = jnp.concatenate([high, low], axis=0)
    sorted_rows[:, width:] = dot_t(place[...], cells).astype(BF16)

    loads["mgain"].wait()
    loads["x"].wait()

    @pl.loop(0, width // 512)
    def _(f):
        cols = pl.ds(pl.multiple_of(f * 512, 512), 512)
        raw[:, cols] = jnp.dot(place[...], x[:, cols], preferred_element_type=F32).astype(BF16)

    def rows_of(ep):
        return pl.ds(pl.multiple_of(ep * rows, rows), rows)

    def normalize(block):
        wide = raw[block, :].astype(F32)
        scale = lax.rsqrt(jnp.mean(wide * wide, axis=-1, keepdims=True) + 1e-06)
        sorted_rows[block, 0:width] = (wide * scale * mgain[...]).astype(BF16)

    def prepare(step):
        normalize(rows_of(pick(leaving, step, peer)))

    prepare(0)
    pl.semaphore_wait(barrier, n_ep - 1 + n_tp - 1)

    others = pl.ds(0, (n_tp - 1) * pad_slot)

    def settle(sem, like):
        pltpu.make_async_copy(like, like, sem).wait()

    def send(src, dst, s_sem, r_sem, ep, tp):
        copy = pltpu.make_async_remote_copy(
            src_ref=src, dst_ref=dst, send_sem=s_sem, recv_sem=r_sem,
            device_id={"ep": ep, "tp": tp}, device_id_type=MESH,
        )
        copy.start()
        return copy

    loads["ig"].wait()
    loads["ci"].wait()
    tail, head = pl.ds(rows_a, HALO), pl.ds(0, HALO)
    halos = [
        pltpu.make_async_remote_copy(
            src_ref=ref.at[tail], dst_ref=ref.at[head], send_sem=h_send, recv_sem=h_recv,
            device_id={"ep": nxt, "tp": me_t}, device_id_type=MESH,
        )
        for ref in (ig, ci)
    ]

    @pl.when(me_e < n_ep - 1)
    def _():
        for copy in halos:
            copy.start()

    def depart(step):
        to, slot = pick(leaving, step, peer), pick(leaving, step)
        send(sorted_rows.at[rows_of(to)], landed.at[slot], d_send, d_recv.at[slot], to, me_t)

    def scatter(step):
        k = pick(coming, step)
        if step:
            settle(d_recv.at[k], landed.at[k])
        chosen = (landed[k, :, pl.ds(width, slots)].astype(F32) != 0.0).astype(BF16)
        picked[k] = tdot(chosen, landed[k, :, 0:width]).astype(BF16)

        def cell(j):
            return pl.ds(pl.multiple_of((k * n_tp + j) * pad_slot, pad_slot), pad_slot)

        for j in range(n_tp - 1, 0, -1):
            to = flip(me_t, j)
            send(
                picked.at[k, pl.ds(pl.multiple_of(to * pad_slot, pad_slot), pad_slot)],
                xin.at[cell(j)], p_send, p_recv.at[k // quarter], me_e, to,
            )
        xin[cell(0), :] = picked[k, pl.ds(pl.multiple_of(me_t * pad_slot, pad_slot), pad_slot), :]


    def conv_ready():
        for name in ("og", "taps", "ggain"):
            loads[name].wait()

        @pl.when(me_e > 0)
        def _():
            settle(h_recv, ig.at[pl.ds(0, 2 * HALO)])

        @pl.when(me_e == 0)
        def _():
            ig[0:HALO, :] = jnp.zeros((HALO, lanes), BF16)

    def conv(j):
        same = (
            lax.broadcasted_iota(jnp.int32, (lanes, lanes), 0) // GROUP_CH
            == lax.broadcasted_iota(jnp.int32, (lanes, lanes), 1) // GROUP_CH
        ).astype(BF16)
        base = pl.multiple_of(flip(me_t, j) * part, part)
        cstep = 64

        @pl.loop(0, part // cstep)
        def _(i):
            at = pl.multiple_of(base + i * cstep, cstep)
            span = pl.ds(at, cstep + HALO)
            product = ig[span, :].astype(F32) * ci[span, :].astype(F32)
            total = taps[reach : reach + 1, :] * product[HALO:, :]
            for back_by in range(1, reach + 1):
                total = total + taps[reach - back_by : reach - back_by + 1, :] * (
                    product[HALO - back_by : HALO - back_by + cstep, :]
                )
            gated[pl.ds(pl.multiple_of(i * cstep, cstep), cstep), :] = (
                og[pl.ds(at, cstep), :].astype(F32) * total
            )

        value = gated[...]
        square = value * value
        s_high = square.astype(BF16)
        s_low = (square - s_high.astype(F32)).astype(BF16)
        mean = (
            jnp.dot(s_high, same, preferred_element_type=F32)
            + jnp.dot(s_low, same, preferred_element_type=F32)
        ) * (1.0 / GROUP_CH)
        done = (value * lax.rsqrt(mean + 1e-06) * ggain[...]).astype(BF16)
        if j:
            normed[pl.ds(base, part), :] = done
        else:
            mixin[0] = done

    def mix_send(j):
        to = flip(me_t, j)
        send(
            normed.at[pl.ds(pl.multiple_of(to * part, part), part)], mixin.at[j],
            m_send, m_recv, me_e, to,
        )

    def mixer():
        settle(m_recv, mixin.at[pl.ds(1, n_tp - 1)])

        @pl.loop(0, width // 512)
        def _(f):
            cols = pl.ds(pl.multiple_of(f * 512, 512), 512)
            total = jnp.zeros((part, 512), F32)
            for j in range(n_tp):
                depth = pl.ds(pl.multiple_of(flip(me_t, j) * lanes, lanes), lanes)
                total = total + jnp.dot(mixin[j], wm[depth, cols], preferred_element_type=F32)
            mixed[:, cols] = total.astype(BF16)

    hid = wg.shape[1]
    mine = pl.ds(pl.multiple_of(me_t * pad_slot, pad_slot), pad_slot)
    here = pl.ds(pl.multiple_of(me_e * rows, rows), rows)

    def rows_in(ks):
        settle(p_recv.at[ks[0] // quarter], xin.at[pl.ds(ks[0] * slots, len(ks) * (n_tp - 1) * pad_slot)])

    def expert(ks):
        first, count = ks[0], len(ks)
        span = pl.ds(first * slots, count * slots)
        hid_rows = pl.ds(0, count * slots)

        @pl.loop(0, hid // 256)
        def _(f):
            cols = pl.ds(pl.multiple_of(f * 256, 256), 256)
            gate = jnp.dot(xin[span, :], wg[:, cols], preferred_element_type=F32)
            up = jnp.dot(xin[span, :], wu[:, cols], preferred_element_type=F32)
            hidden[hid_rows, cols] = (gate / (1.0 + jnp.exp(-gate)) * up).astype(BF16)

        @pl.loop(0, width // 512)
        def _(f):
            cols = pl.ds(pl.multiple_of(f * 512, 512), 512)
            xin[span, cols] = jnp.dot(
                hidden[hid_rows, :], wd[:, cols], preferred_element_type=F32
            ).astype(BF16)

    def give_back(ks):
        for k in ks:
            for j in range(n_tp - 1, 0, -1):
                send(
                    xin.at[pl.ds((k * n_tp + j) * pad_slot, pad_slot)],
                    comb.at[k, mine], r_send, r_recv.at[k], me_e, flip(me_t, j),
                )
            comb[k, mine, :] = xin[pl.ds(k * slots, pad_slot), :]


    def combine(k):
        settle(r_recv.at[k], comb.at[k, others])
        total = jnp.dot(
            landed[k, :, pl.ds(width, slots)], comb[k], preferred_element_type=F32
        ) + jnp.dot(
            landed[k, :, pl.ds(width + slots, slots)], comb[k], preferred_element_type=F32
        )
        if k == 0:
            fin[here, :] = total.astype(BF16)
            return
        sums[k] = total.astype(BF16)
        send(sums.at[k], fin.at[here], f_send, f_recv, flip(me_e, k), me_t)

    half = n_ep // 2
    depart(0)
    for step in range(1, n_ep):
        prepare(step)
        if step == quarter:
            landed[0] = sorted_rows[rows_of(me_e), :]
            scatter(0)
        else:
            depart(step)
    conv_ready()
    conv(n_tp - 1)
    mix_send(n_tp - 1)
    for j in range(n_tp - 2, -1, -1):
        conv(j)
    mix_send(1)
    for k in q0[1:]:
        scatter(k)
    for k in q1[:split]:
        scatter(k)
    for k in q1[split:]:
        scatter(k)
    for k in q2[:split]:
        scatter(k)
    for name in ("wg", "wu", "wd"):
        loads[name].wait()
    rows_in(q0)
    for k in q2[split:]:
        scatter(k)
    for j in range(n_tp - 2, 1, -1):
        mix_send(j)
    rows_in(q2)
    for k in q3[:split]:
        scatter(k)
    expert(q2)
    give_back(q2[:split])
    rows_in(q1)
    for k in q3[split:]:
        scatter(k)
    give_back(q2[split:])
    expert(q1)
    give_back(q1[split:])
    for k in q2[:split]:
        combine(k)
    loads["wm"].wait()
    mixer()
    rows_in(q3)
    expert(q3)
    for k in q2[split:]:
        combine(k)
    give_back(q3[split:])
    for k in q1[split:]:
        combine(k)
    give_back(q1[:split])
    give_back(q3[:split])
    for k in q3[split:]:
        combine(k)
    expert(q0)
    give_back(q0[split:])
    for k in q1[:split]:
        combine(k)
    give_back(q0[:split])
    for k in q3[:split]:
        combine(k)
    for k in q0[split:]:
        combine(k)
    for k in q0[:split]:
        combine(k)
    settle(f_recv, fin.at[pl.ds(0, (n_ep - 1) * rows)])
    @pl.when(me_e < n_ep - 1)
    def _():
        settle(h_send, ig.at[pl.ds(0, 2 * HALO)])

    settle(d_send, sorted_rows.at[pl.ds(0, (n_ep - 1) * rows)])
    settle(m_send, normed.at[pl.ds(0, (n_tp - 1) * part)])
    settle(p_send, picked.at[:, others])
    settle(r_send, comb.at[:, others])
    settle(f_send, sums.at[pl.ds(0, n_ep - 1)])


def layer(
    out_gate, in_gate, conv_input, conv_taps, group_gain, mix_out_w,
    moe_in, moe_gain, route_ids, route_weight, gate_w, up_w, down_w,
):
    n_ep, n_tp = lax.axis_size("ep"), lax.axis_size("tp")
    tok, width = moe_in.shape
    hid = gate_w.shape[2]
    pad_slot = round_up(2 * tok // (n_ep * n_tp), 16)
    rows = tok // n_ep
    slots = n_tp * pad_slot
    meta = round_up(2 * slots, 128)
    total = n_ep * slots
    rows_a, lanes = out_gate.shape
    part = rows_a // n_tp
    channels = mix_out_w.shape[0]
    taps = conv_taps.shape[0]
    hbm = pl.BlockSpec(memory_space=pltpu.HBM)
    dma = pltpu.SemaphoreType.DMA
    vm = pltpu.VMEM
    scratch = [
        vm((rows_a, lanes), BF16),
        vm((HALO + rows_a, lanes), BF16),
        vm((HALO + rows_a, lanes), BF16),
        vm((taps, lanes), F32),
        vm((1, lanes), F32),
        vm((channels, width), BF16),
        vm((tok, width), BF16),
        vm((1, width), F32),
        vm((2, tok), jnp.int32),
        vm((2, tok), F32),
        vm((width, hid), BF16),
        vm((width, hid), BF16),
        vm((hid, width), BF16),
        vm((rows_a, lanes), BF16),
        vm((part, lanes), F32),
        vm((tok, width), BF16),
        vm((tok, width + meta), BF16),
        vm((n_ep, rows, width + meta), BF16),
        vm((n_ep, slots, width), BF16),
        vm((total, width), BF16),
        vm((total // 4, hid), BF16),
        vm((n_ep, slots, width), BF16),
        vm((n_ep, rows, width), BF16),
        vm((n_tp, part, lanes), BF16),
        dma((13,)),
        dma(()),
        dma(()),
        dma(()),
        dma(()),
        dma(()),
        dma((n_ep,)),
        dma(()),
        dma((4,)),
        dma(()),
        dma((n_ep,)),
        dma(()),
        dma(()),
    ]
    held = 2 * (part * width + tok * width + tok * tok) + sum(
        math.prod(one.shape) * jnp.dtype(one.dtype).itemsize for one in scratch if one.memory_space == vm
    )
    return pl.pallas_call(
        functools.partial(layer_kernel, n_ep, n_tp, pad_slot, taps - 1),
        out_shape=[
            jax.ShapeDtypeStruct((part, width), BF16),
            jax.ShapeDtypeStruct((tok, width), BF16),
            jax.ShapeDtypeStruct((tok, tok), BF16),
        ],
        in_specs=[hbm] * 13,
        out_specs=[pl.BlockSpec(memory_space=vm)] * 3,
        scratch_shapes=scratch,
        compiler_params=pltpu.CompilerParams(
            collective_id=0, has_side_effects=True, vmem_limit_bytes=min(held + SPARE, VMEM_BYTES)
        ),
        cost_estimate=pl.CostEstimate(
            flops=6 * total * width * hid, bytes_accessed=8 * width * hid, transcendentals=0
        ),
    )(*[pltpu.with_memory_space_constraint(a, pltpu.HBM) for a in (
        out_gate, in_gate, conv_input, conv_taps, group_gain.reshape(1, lanes), mix_out_w,
        moe_in, moe_gain.reshape(1, width), route_ids.T, route_weight.T, gate_w, up_w, down_w,
    )])


def finish_kernel(mixed_in, fin, place, mixed, out, done, sem):
    copies = [pltpu.make_async_copy(mixed_in, mixed, sem.at[0])]
    copies[0].start()
    block = 512
    for i in range(done.shape[1] // block):
        cols = pl.ds(i * block, block)
        done[:, cols] = tdot(place[...], fin[:, cols]).astype(BF16)
        copies.append(pltpu.make_async_copy(done.at[:, cols], out.at[:, cols], sem.at[1 + i]))
        copies[-1].start()
    for copy in copies:
        copy.wait()


def shards(*args):
    mixed, fin, place = layer(*args)
    tok, width = fin.shape
    vm = pl.BlockSpec(memory_space=pltpu.VMEM)
    hbm = pl.BlockSpec(memory_space=pl.ANY)
    return pl.pallas_call(
        finish_kernel,
        out_shape=[
            jax.ShapeDtypeStruct(mixed.shape, BF16),
            jax.ShapeDtypeStruct((tok, width), BF16),
        ],
        in_specs=[vm, vm, vm],
        out_specs=[hbm, hbm],
        scratch_shapes=[pltpu.VMEM((tok, width), BF16), pltpu.SemaphoreType.DMA((1 + width // 512,))],
        compiler_params=pltpu.CompilerParams(vmem_limit_bytes=8 << 20),
        cost_estimate=pl.CostEstimate(
            flops=2 * tok * tok * width, bytes_accessed=8 * tok * width, transcendentals=0
        ),
    )(mixed, fin, place)


def solution(mesh):
    in_specs = (
        P("ep", "tp"),
        P("ep", "tp"),
        P("ep", "tp"),
        P(None, "tp"),
        P("tp"),
        P(),
        P(("ep", "tp"), None),
        P(),
        P(("ep", "tp"), None),
        P(("ep", "tp"), None),
        P(("ep", "tp"), None, None),
        P(("ep", "tp"), None, None),
        P(("ep", "tp"), None, None),
    )
    out_specs = (P(("ep", "tp"), None), P(("ep", "tp"), None))
    return jax.shard_map(shards, mesh=mesh, in_specs=in_specs, out_specs=out_specs, check_vma=False)
```

```python
import functools
import math

import jax
import jax.numpy as jnp
from jax import lax
from jax.experimental import pallas as pl
from jax.experimental.pallas import tpu as pltpu
from jax.sharding import PartitionSpec as P

GROUP_CH = 64
HALO = 16
VMEM_BYTES = 60 * 1024 * 1024
SPARE = 6 << 20
MESH = pl.DeviceIdType.MESH
BF16 = jnp.bfloat16
F32 = jnp.float32


def round_up(value, to):
    return (value + to - 1) // to * to


def tdot(a, b):
    return lax.dot_general(a, b, (((0,), (0,)), ((), ())), preferred_element_type=F32)


def dot_t(a, b):
    return lax.dot_general(a, b, (((1,), (1,)), ((), ())), preferred_element_type=F32)


def flip(index, mask):
    bit = 1
    out = index
    while bit <= mask:
        if mask & bit:
            out = out + bit * (1 - 2 * ((index // bit) % 2))
        bit *= 2
    return out


def layer_kernel(
    n_ep, n_tp, pad_slot, reach,
    og_hbm, ig_hbm, ci_hbm, taps_hbm, ggain_hbm, wm_hbm,
    x_hbm, mgain_hbm, ids_hbm, rw_hbm, wg_hbm, wu_hbm, wd_hbm,
    mixed, fin, place,
    og, ig, ci, taps, ggain, wm, x, mgain, ids, rw, wg, wu, wd,
    normed, gated, raw, sorted_rows, landed, picked, xin, hidden, comb, sums, mixin,
    in_sem, h_send, h_recv, m_send, m_recv, d_send, d_recv, p_send, p_recv, r_send, r_recv, f_send, f_recv,
):
    me_e = lax.axis_index("ep")
    me_t = lax.axis_index("tp")
    tok, width = x.shape
    rows = tok // n_ep
    slots = n_tp * pad_slot
    experts = n_ep * n_tp
    rows_a, lanes = og.shape
    part = rows_a // n_tp
    quarter = n_ep // 4
    q0, q1, q2, q3 = [list(range(i * quarter, (i + 1) * quarter)) for i in range(4)]

    middle = ((me_e // quarter + 1) // 2) % 2
    split = quarter // 2
    leaving = q1 + q0 + q2 + q3, q2 + q0 + q1 + q3
    coming = q0 + q2[:split] + q1 + q2[split:] + q3, q0 + q1 + q2 + q3

    def pick(orders, step, of=lambda k: k):
        outer, inner = orders[0][step], orders[1][step]
        if outer == inner:
            return of(outer)
        return middle * of(inner) + (1 - middle) * of(outer)

    def peer(k):
        return flip(me_e, k)

    barrier = pltpu.get_barrier_semaphore()
    for k in range(1, n_ep):
        pl.semaphore_signal(
            barrier, inc=1, device_id={"ep": flip(me_e, k), "tp": me_t}, device_id_type=MESH
        )
    for j in range(1, n_tp):
        pl.semaphore_signal(
            barrier, inc=1, device_id={"ep": me_e, "tp": flip(me_t, j)}, device_id_type=MESH
        )
    nxt = lax.rem(me_e + 1, n_ep)
    own = pl.ds(HALO, rows_a)
    loads = {}
    for i, (name, src, dst) in enumerate((
        ("ids", ids_hbm, ids), ("rw", rw_hbm, rw), ("mgain", mgain_hbm, mgain), ("x", x_hbm, x),
        ("ig", ig_hbm, ig.at[own]), ("ci", ci_hbm, ci.at[own]), ("og", og_hbm, og),
        ("taps", taps_hbm, taps), ("ggain", ggain_hbm, ggain),
        ("wg", wg_hbm.at[0], wg), ("wu", wu_hbm.at[0], wu), ("wd", wd_hbm.at[0], wd), ("wm", wm_hbm, wm),
    )):
        loads[name] = pltpu.make_async_copy(src, dst, in_sem.at[i])
        loads[name].start()

    loads["ids"].wait()
    loads["rw"].wait()
    ids0, ids1 = ids[0:1, :], ids[1:2, :]
    sub_e = lax.broadcasted_iota(jnp.int32, (experts, tok), 0)
    hit0 = (ids0 == sub_e).astype(F32)
    hit1 = (ids1 == sub_e).astype(F32)
    both = (hit0 + hit1).astype(BF16)
    upper = (
        lax.broadcasted_iota(jnp.int32, (tok, tok), 0) < lax.broadcasted_iota(jnp.int32, (tok, tok), 1)
    ).astype(BF16)
    before = jnp.dot(both, upper, preferred_element_type=F32)
    rank0 = jnp.sum(before * hit0, axis=0, keepdims=True).astype(jnp.int32)
    rank1 = jnp.sum(before * hit1, axis=0, keepdims=True).astype(jnp.int32)
    group = ids0 // n_tp
    in_group = (group == (sub_e // n_tp)).astype(F32)
    rank_g = jnp.sum(before * in_group, axis=0, keepdims=True).astype(jnp.int32) // 2
    place[...] = (
        (group * rows + rank_g) == lax.broadcasted_iota(jnp.int32, (tok, tok), 0)
    ).astype(BF16)
    cell0 = (ids0 - group * n_tp) * pad_slot + rank0
    cell1 = (ids1 - group * n_tp) * pad_slot + rank1
    sub_s = lax.broadcasted_iota(jnp.int32, (slots, tok), 0)
    weight = jnp.where(cell0 == sub_s, rw[0:1, :], 0.0) + jnp.where(cell1 == sub_s, rw[1:2, :], 0.0)
    high = weight.astype(BF16)
    low = (weight - high.astype(F32)).astype(BF16)
    cells = jnp.concatenate([high, low], axis=0)
    sorted_rows[:, width:] = dot_t(place[...], cells).astype(BF16)

    loads["mgain"].wait()
    loads["x"].wait()

    @pl.loop(0, width // 512)
    def _(f):
        cols = pl.ds(pl.multiple_of(f * 512, 512), 512)
        raw[:, cols] = jnp.dot(place[...], x[:, cols], preferred_element_type=F32).astype(BF16)

    def rows_of(ep):
        return pl.ds(pl.multiple_of(ep * rows, rows), rows)

    def normalize(block):
        wide = raw[block, :].astype(F32)
        scale = lax.rsqrt(jnp.mean(wide * wide, axis=-1, keepdims=True) + 1e-06)
        sorted_rows[block, 0:width] = (wide * scale * mgain[...]).astype(BF16)

    def prepare(step):
        normalize(rows_of(pick(leaving, step, peer)))

    prepare(0)
    pl.semaphore_wait(barrier, n_ep - 1 + n_tp - 1)

    others = pl.ds(0, (n_tp - 1) * pad_slot)

    def settle(sem, like):
        pltpu.make_async_copy(like, like, sem).wait()

    def send(src, dst, s_sem, r_sem, ep, tp):
        copy = pltpu.make_async_remote_copy(
            src_ref=src, dst_ref=dst, send_sem=s_sem, recv_sem=r_sem,
            device_id={"ep": ep, "tp": tp}, device_id_type=MESH,
        )
        copy.start()
        return copy

    loads["ig"].wait()
    loads["ci"].wait()
    tail, head = pl.ds(rows_a, HALO), pl.ds(0, HALO)
    halos = [
        pltpu.make_async_remote_copy(
            src_ref=ref.at[tail], dst_ref=ref.at[head], send_sem=h_send, recv_sem=h_recv,
            device_id={"ep": nxt, "tp": me_t}, device_id_type=MESH,
        )
        for ref in (ig, ci)
    ]

    @pl.when(me_e < n_ep - 1)
    def _():
        for copy in halos:
            copy.start()

    def depart(step):
        to, slot = pick(leaving, step, peer), pick(leaving, step)
        send(sorted_rows.at[rows_of(to)], landed.at[slot], d_send, d_recv.at[slot], to, me_t)

    def scatter(step):
        k = pick(coming, step)
        if step:
            settle(d_recv.at[k], landed.at[k])
        chosen = (landed[k, :, pl.ds(width, slots)].astype(F32) != 0.0).astype(BF16)
        picked[k] = tdot(chosen, landed[k, :, 0:width]).astype(BF16)

        def cell(j):
            return pl.ds(pl.multiple_of((k * n_tp + j) * pad_slot, pad_slot), pad_slot)

        for j in range(n_tp - 1, 0, -1):
            to = flip(me_t, j)
            send(
                picked.at[k, pl.ds(pl.multiple_of(to * pad_slot, pad_slot), pad_slot)],
                xin.at[cell(j)], p_send, p_recv.at[k // quarter], me_e, to,
            )
        xin[cell(0), :] = picked[k, pl.ds(pl.multiple_of(me_t * pad_slot, pad_slot), pad_slot), :]


    def conv_ready():
        for name in ("og", "taps", "ggain"):
            loads[name].wait()

        @pl.when(me_e > 0)
        def _():
            settle(h_recv, ig.at[pl.ds(0, 2 * HALO)])

        @pl.when(me_e == 0)
        def _():
            ig[0:HALO, :] = jnp.zeros((HALO, lanes), BF16)

    def conv(j):
        same = (
            lax.broadcasted_iota(jnp.int32, (lanes, lanes), 0) // GROUP_CH
            == lax.broadcasted_iota(jnp.int32, (lanes, lanes), 1) // GROUP_CH
        ).astype(BF16)
        base = pl.multiple_of(flip(me_t, j) * part, part)
        cstep = 64

        @pl.loop(0, part // cstep)
        def _(i):
            at = pl.multiple_of(base + i * cstep, cstep)
            span = pl.ds(at, cstep + HALO)
            product = ig[span, :].astype(F32) * ci[span, :].astype(F32)
            total = taps[reach : reach + 1, :] * product[HALO:, :]
            for back_by in range(1, reach + 1):
                total = total + taps[reach - back_by : reach - back_by + 1, :] * (
                    product[HALO - back_by : HALO - back_by + cstep, :]
                )
            gated[pl.ds(pl.multiple_of(i * cstep, cstep), cstep), :] = (
                og[pl.ds(at, cstep), :].astype(F32) * total
            )

        value = gated[...]
        square = value * value
        s_high = square.astype(BF16)
        s_low = (square - s_high.astype(F32)).astype(BF16)
        mean = (
            jnp.dot(s_high, same, preferred_element_type=F32)
            + jnp.dot(s_low, same, preferred_element_type=F32)
        ) * (1.0 / GROUP_CH)
        done = (value * lax.rsqrt(mean + 1e-06) * ggain[...]).astype(BF16)
        if j:
            normed[pl.ds(base, part), :] = done
        else:
            mixin[0] = done

    def mix_send(j):
        to = flip(me_t, j)
        send(
            normed.at[pl.ds(pl.multiple_of(to * part, part), part)], mixin.at[j],
            m_send, m_recv, me_e, to,
        )

    def mixer():
        settle(m_recv, mixin.at[pl.ds(1, n_tp - 1)])

        for f in range(width // 512):
            cols = pl.ds(f * 512, 512)
            total = jnp.zeros((part, 512), F32)
            for j in range(n_tp):
                depth = pl.ds(pl.multiple_of(flip(me_t, j) * lanes, lanes), lanes)
                total = total + jnp.dot(mixin[j], wm[depth, cols], preferred_element_type=F32)
            mixed[:, cols] = total.astype(BF16)

    hid = wg.shape[1]
    mine = pl.ds(pl.multiple_of(me_t * pad_slot, pad_slot), pad_slot)
    here = pl.ds(pl.multiple_of(me_e * rows, rows), rows)

    def rows_in(ks):
        settle(p_recv.at[ks[0] // quarter], xin.at[pl.ds(ks[0] * slots, len(ks) * (n_tp - 1) * pad_slot)])

    def expert(ks):
        first, count = ks[0], len(ks)
        span = pl.ds(first * slots, count * slots)
        hid_rows = pl.ds(0, count * slots)

        for f in range(hid // 256):
            cols = pl.ds(f * 256, 256)
            gate = jnp.dot(xin[span, :], wg[:, cols], preferred_element_type=F32)
            up = jnp.dot(xin[span, :], wu[:, cols], preferred_element_type=F32)
            hidden[hid_rows, cols] = (gate / (1.0 + jnp.exp(-gate)) * up).astype(BF16)

        for f in range(width // 512):
            cols = pl.ds(f * 512, 512)
            xin[span, cols] = jnp.dot(
                hidden[hid_rows, :], wd[:, cols], preferred_element_type=F32
            ).astype(BF16)

    def give_back(ks):
        for k in ks:
            for j in range(n_tp - 1, 0, -1):
                send(
                    xin.at[pl.ds((k * n_tp + j) * pad_slot, pad_slot)],
                    comb.at[k, mine], r_send, r_recv.at[k], me_e, flip(me_t, j),
                )
            comb[k, mine, :] = xin[pl.ds(k * slots, pad_slot), :]


    def combine(k):
        settle(r_recv.at[k], comb.at[k, others])
        total = jnp.dot(
            landed[k, :, pl.ds(width, slots)], comb[k], preferred_element_type=F32
        ) + jnp.dot(
            landed[k, :, pl.ds(width + slots, slots)], comb[k], preferred_element_type=F32
        )
        if k == 0:
            fin[here, :] = total.astype(BF16)
            return
        sums[k] = total.astype(BF16)
        send(sums.at[k], fin.at[here], f_send, f_recv, flip(me_e, k), me_t)

    half = n_ep // 2
    depart(0)
    for step in range(1, n_ep):
        prepare(step)
        if step == quarter:
            landed[0] = sorted_rows[rows_of(me_e), :]
            scatter(0)
        else:
            depart(step)
    conv_ready()
    conv(n_tp - 1)
    mix_send(n_tp - 1)
    for j in range(n_tp - 2, -1, -1):
        conv(j)
    mix_send(1)
    for k in q0[1:]:
        scatter(k)
    for k in q1[:split]:
        scatter(k)
    for k in q1[split:]:
        scatter(k)
    for k in q2[:split]:
        scatter(k)
    for name in ("wg", "wu", "wd"):
        loads[name].wait()
    rows_in(q0)
    for k in q2[split:]:
        scatter(k)
    for j in range(n_tp - 2, 1, -1):
        mix_send(j)
    rows_in(q2)
    for k in q3[:split]:
        scatter(k)
    expert(q2)
    give_back(q2[:split])
    rows_in(q1)
    for k in q3[split:]:
        scatter(k)
    give_back(q2[split:])
    expert(q1)
    give_back(q1[split:])
    for k in q2[:split]:
        combine(k)
    loads["wm"].wait()
    mixer()
    rows_in(q3)
    expert(q3)
    for k in q2[split:]:
        combine(k)
    give_back(q3[split:])
    for k in q1[split:]:
        combine(k)
    give_back(q1[:split])
    give_back(q3[:split])
    for k in q3[split:]:
        combine(k)
    expert(q0)
    give_back(q0[split:])
    for k in q1[:split]:
        combine(k)
    give_back(q0[:split])
    for k in q3[:split]:
        combine(k)
    for k in q0[split:]:
        combine(k)
    for k in q0[:split]:
        combine(k)
    settle(f_recv, fin.at[pl.ds(0, (n_ep - 1) * rows)])
    @pl.when(me_e < n_ep - 1)
    def _():
        settle(h_send, ig.at[pl.ds(0, 2 * HALO)])

    settle(d_send, sorted_rows.at[pl.ds(0, (n_ep - 1) * rows)])
    settle(m_send, normed.at[pl.ds(0, (n_tp - 1) * part)])
    settle(p_send, picked.at[:, others])
    settle(r_send, comb.at[:, others])
    settle(f_send, sums.at[pl.ds(0, n_ep - 1)])


def layer(
    out_gate, in_gate, conv_input, conv_taps, group_gain, mix_out_w,
    moe_in, moe_gain, route_ids, route_weight, gate_w, up_w, down_w,
):
    n_ep, n_tp = lax.axis_size("ep"), lax.axis_size("tp")
    tok, width = moe_in.shape
    hid = gate_w.shape[2]
    pad_slot = round_up(2 * tok // (n_ep * n_tp), 16)
    rows = tok // n_ep
    slots = n_tp * pad_slot
    meta = round_up(2 * slots, 128)
    total = n_ep * slots
    rows_a, lanes = out_gate.shape
    part = rows_a // n_tp
    channels = mix_out_w.shape[0]
    taps = conv_taps.shape[0]
    hbm = pl.BlockSpec(memory_space=pltpu.HBM)
    dma = pltpu.SemaphoreType.DMA
    vm = pltpu.VMEM
    scratch = [
        vm((rows_a, lanes), BF16),
        vm((HALO + rows_a, lanes), BF16),
        vm((HALO + rows_a, lanes), BF16),
        vm((taps, lanes), F32),
        vm((1, lanes), F32),
        vm((channels, width), BF16),
        vm((tok, width), BF16),
        vm((1, width), F32),
        vm((2, tok), jnp.int32),
        vm((2, tok), F32),
        vm((width, hid), BF16),
        vm((width, hid), BF16),
        vm((hid, width), BF16),
        vm((rows_a, lanes), BF16),
        vm((part, lanes), F32),
        vm((tok, width), BF16),
        vm((tok, width + meta), BF16),
        vm((n_ep, rows, width + meta), BF16),
        vm((n_ep, slots, width), BF16),
        vm((total, width), BF16),
        vm((total // 4, hid), BF16),
        vm((n_ep, slots, width), BF16),
        vm((n_ep, rows, width), BF16),
        vm((n_tp, part, lanes), BF16),
        dma((13,)),
        dma(()),
        dma(()),
        dma(()),
        dma(()),
        dma(()),
        dma((n_ep,)),
        dma(()),
        dma((4,)),
        dma(()),
        dma((n_ep,)),
        dma(()),
        dma(()),
    ]
    held = 2 * (part * width + tok * width + tok * tok) + sum(
        math.prod(one.shape) * jnp.dtype(one.dtype).itemsize for one in scratch if one.memory_space == vm
    )
    return pl.pallas_call(
        functools.partial(layer_kernel, n_ep, n_tp, pad_slot, taps - 1),
        out_shape=[
            jax.ShapeDtypeStruct((part, width), BF16),
            jax.ShapeDtypeStruct((tok, width), BF16),
            jax.ShapeDtypeStruct((tok, tok), BF16),
        ],
        in_specs=[hbm] * 13,
        out_specs=[pl.BlockSpec(memory_space=vm)] * 3,
        scratch_shapes=scratch,
        compiler_params=pltpu.CompilerParams(
            collective_id=0, has_side_effects=True, vmem_limit_bytes=min(held + SPARE, VMEM_BYTES)
        ),
        cost_estimate=pl.CostEstimate(
            flops=6 * total * width * hid, bytes_accessed=8 * width * hid, transcendentals=0
        ),
    )(*[pltpu.with_memory_space_constraint(a, pltpu.HBM) for a in (
        out_gate, in_gate, conv_input, conv_taps, group_gain.reshape(1, lanes), mix_out_w,
        moe_in, moe_gain.reshape(1, width), route_ids.T, route_weight.T, gate_w, up_w, down_w,
    )])


def finish_kernel(mixed_in, fin, place, mixed, out, done, sem):
    copies = [pltpu.make_async_copy(mixed_in, mixed, sem.at[0])]
    copies[0].start()
    block = 512
    for i in range(done.shape[1] // block):
        cols = pl.ds(i * block, block)
        done[:, cols] = tdot(place[...], fin[:, cols]).astype(BF16)
        copies.append(pltpu.make_async_copy(done.at[:, cols], out.at[:, cols], sem.at[1 + i]))
        copies[-1].start()
    for copy in copies:
        copy.wait()


def shards(*args):
    mixed, fin, place = layer(*args)
    tok, width = fin.shape
    vm = pl.BlockSpec(memory_space=pltpu.VMEM)
    hbm = pl.BlockSpec(memory_space=pl.ANY)
    return pl.pallas_call(
        finish_kernel,
        out_shape=[
            jax.ShapeDtypeStruct(mixed.shape, BF16),
            jax.ShapeDtypeStruct((tok, width), BF16),
        ],
        in_specs=[vm, vm, vm],
        out_specs=[hbm, hbm],
        scratch_shapes=[pltpu.VMEM((tok, width), BF16), pltpu.SemaphoreType.DMA((1 + width // 512,))],
        compiler_params=pltpu.CompilerParams(vmem_limit_bytes=8 << 20),
        cost_estimate=pl.CostEstimate(
            flops=2 * tok * tok * width, bytes_accessed=8 * tok * width, transcendentals=0
        ),
    )(mixed, fin, place)


def solution(mesh):
    in_specs = (
        P("ep", "tp"),
        P("ep", "tp"),
        P("ep", "tp"),
        P(None, "tp"),
        P("tp"),
        P(),
        P(("ep", "tp"), None),
        P(),
        P(("ep", "tp"), None),
        P(("ep", "tp"), None),
        P(("ep", "tp"), None, None),
        P(("ep", "tp"), None, None),
        P(("ep", "tp"), None, None),
    )
    out_specs = (P(("ep", "tp"), None), P(("ep", "tp"), None))
    return jax.shard_map(shards, mesh=mesh, in_specs=in_specs, out_specs=out_specs, check_vma=False)
```

```python
import functools
import math

import jax
import jax.numpy as jnp
from jax import lax
from jax.experimental import pallas as pl
from jax.experimental.pallas import tpu as pltpu
from jax.sharding import PartitionSpec as P

GROUP_CH = 64
HALO = 16
VMEM_BYTES = 60 * 1024 * 1024
SPARE = 6 << 20
MESH = pl.DeviceIdType.MESH
BF16 = jnp.bfloat16
F32 = jnp.float32


def round_up(value, to):
    return (value + to - 1) // to * to


def tdot(a, b):
    return lax.dot_general(a, b, (((0,), (0,)), ((), ())), preferred_element_type=F32)


def dot_t(a, b):
    return lax.dot_general(a, b, (((1,), (1,)), ((), ())), preferred_element_type=F32)


def flip(index, mask):
    bit = 1
    out = index
    while bit <= mask:
        if mask & bit:
            out = out + bit * (1 - 2 * ((index // bit) % 2))
        bit *= 2
    return out


def layer_kernel(
    n_ep, n_tp, pad_slot, reach,
    og_hbm, ig_hbm, ci_hbm, taps_hbm, ggain_hbm, wm_hbm,
    x_hbm, mgain_hbm, ids_hbm, rw_hbm, wg_hbm, wu_hbm, wd_hbm,
    mixed, fin, place,
    og, ig, ci, taps, ggain, wm, x, mgain, ids, rw, wg, wu, wd,
    normed, gated, raw, sorted_rows, landed, picked, xin, hidden, comb, sums, mixin,
    in_sem, h_send, h_recv, m_send, m_recv, d_send, d_recv, p_send, p_recv, r_send, r_recv, f_send, f_recv,
):
    me_e = lax.axis_index("ep")
    me_t = lax.axis_index("tp")
    tok, width = x.shape
    rows = tok // n_ep
    slots = n_tp * pad_slot
    experts = n_ep * n_tp
    rows_a, lanes = og.shape
    part = rows_a // n_tp
    quarter = n_ep // 4
    q0, q1, q2, q3 = [list(range(i * quarter, (i + 1) * quarter)) for i in range(4)]

    middle = ((me_e // quarter + 1) // 2) % 2
    split = quarter // 2
    leaving = q1 + q0 + q2 + q3, q2 + q0 + q1 + q3
    coming = q0 + q2[:split] + q1 + q2[split:] + q3, q0 + q1 + q2 + q3

    def pick(orders, step, of=lambda k: k):
        outer, inner = orders[0][step], orders[1][step]
        if outer == inner:
            return of(outer)
        return middle * of(inner) + (1 - middle) * of(outer)

    def peer(k):
        return flip(me_e, k)

    barrier = pltpu.get_barrier_semaphore()
    for k in range(1, n_ep):
        pl.semaphore_signal(
            barrier, inc=1, device_id={"ep": flip(me_e, k), "tp": me_t}, device_id_type=MESH
        )
    for j in range(1, n_tp):
        pl.semaphore_signal(
            barrier, inc=1, device_id={"ep": me_e, "tp": flip(me_t, j)}, device_id_type=MESH
        )
    nxt = lax.rem(me_e + 1, n_ep)
    own = pl.ds(HALO, rows_a)
    loads = {}
    for i, (name, src, dst) in enumerate((
        ("ids", ids_hbm, ids), ("rw", rw_hbm, rw), ("mgain", mgain_hbm, mgain), ("x", x_hbm, x),
        ("ig", ig_hbm, ig.at[own]), ("ci", ci_hbm, ci.at[own]), ("og", og_hbm, og),
        ("taps", taps_hbm, taps), ("ggain", ggain_hbm, ggain),
        ("wg", wg_hbm.at[0], wg), ("wu", wu_hbm.at[0], wu), ("wd", wd_hbm.at[0], wd), ("wm", wm_hbm, wm),
    )):
        loads[name] = pltpu.make_async_copy(src, dst, in_sem.at[i])
        loads[name].start()

    loads["ids"].wait()
    loads["rw"].wait()
    ids0, ids1 = ids[0:1, :], ids[1:2, :]
    sub_e = lax.broadcasted_iota(jnp.int32, (experts, tok), 0)
    hit0 = (ids0 == sub_e).astype(F32)
    hit1 = (ids1 == sub_e).astype(F32)
    both = (hit0 + hit1).astype(BF16)
    upper = (
        lax.broadcasted_iota(jnp.int32, (tok, tok), 0) < lax.broadcasted_iota(jnp.int32, (tok, tok), 1)
    ).astype(BF16)
    before = jnp.dot(both, upper, preferred_element_type=F32)
    rank0 = jnp.sum(before * hit0, axis=0, keepdims=True).astype(jnp.int32)
    rank1 = jnp.sum(before * hit1, axis=0, keepdims=True).astype(jnp.int32)
    group = ids0 // n_tp
    in_group = (group == (sub_e // n_tp)).astype(F32)
    rank_g = jnp.sum(before * in_group, axis=0, keepdims=True).astype(jnp.int32) // 2
    place[...] = (
        (group * rows + rank_g) == lax.broadcasted_iota(jnp.int32, (tok, tok), 0)
    ).astype(BF16)
    cell0 = (ids0 - group * n_tp) * pad_slot + rank0
    cell1 = (ids1 - group * n_tp) * pad_slot + rank1
    sub_s = lax.broadcasted_iota(jnp.int32, (slots, tok), 0)
    weight = jnp.where(cell0 == sub_s, rw[0:1, :], 0.0) + jnp.where(cell1 == sub_s, rw[1:2, :], 0.0)
    high = weight.astype(BF16)
    low = (weight - high.astype(F32)).astype(BF16)
    cells = jnp.concatenate([high, low], axis=0)
    sorted_rows[:, width:] = dot_t(place[...], cells).astype(BF16)

    loads["mgain"].wait()
    loads["x"].wait()

    @pl.loop(0, width // 512)
    def _(f):
        cols = pl.ds(pl.multiple_of(f * 512, 512), 512)
        raw[:, cols] = jnp.dot(place[...], x[:, cols], preferred_element_type=F32).astype(BF16)

    def rows_of(ep):
        return pl.ds(pl.multiple_of(ep * rows, rows), rows)

    def normalize(block):
        wide = raw[block, :].astype(F32)
        scale = lax.rsqrt(jnp.mean(wide * wide, axis=-1, keepdims=True) + 1e-06)
        sorted_rows[block, 0:width] = (wide * scale * mgain[...]).astype(BF16)

    def prepare(step):
        normalize(rows_of(pick(leaving, step, peer)))

    normalize(rows_of(me_e))
    landed[0] = sorted_rows[rows_of(me_e), :]

    def sort_out(k):
        chosen = (landed[k, :, pl.ds(width, slots)].astype(F32) != 0.0).astype(BF16)
        picked[k] = tdot(chosen, landed[k, :, 0:width]).astype(BF16)

    sort_out(0)
    for step in range(quarter):
        prepare(step)
    pl.semaphore_wait(barrier, n_ep - 1 + n_tp - 1)

    others = pl.ds(0, (n_tp - 1) * pad_slot)

    def settle(sem, like):
        pltpu.make_async_copy(like, like, sem).wait()

    def send(src, dst, s_sem, r_sem, ep, tp):
        copy = pltpu.make_async_remote_copy(
            src_ref=src, dst_ref=dst, send_sem=s_sem, recv_sem=r_sem,
            device_id={"ep": ep, "tp": tp}, device_id_type=MESH,
        )
        copy.start()
        return copy

    loads["ig"].wait()
    loads["ci"].wait()
    tail, head = pl.ds(rows_a, HALO), pl.ds(0, HALO)
    halos = [
        pltpu.make_async_remote_copy(
            src_ref=ref.at[tail], dst_ref=ref.at[head], send_sem=h_send, recv_sem=h_recv,
            device_id={"ep": nxt, "tp": me_t}, device_id_type=MESH,
        )
        for ref in (ig, ci)
    ]

    @pl.when(me_e < n_ep - 1)
    def _():
        for copy in halos:
            copy.start()

    def depart(step):
        to, slot = pick(leaving, step, peer), pick(leaving, step)
        send(sorted_rows.at[rows_of(to)], landed.at[slot], d_send, d_recv.at[slot], to, me_t)

    def scatter(step):
        k = pick(coming, step)
        if step:
            settle(d_recv.at[k], landed.at[k])
            sort_out(k)

        def cell(j):
            return pl.ds(pl.multiple_of((k * n_tp + j) * pad_slot, pad_slot), pad_slot)

        for j in range(n_tp - 1, 0, -1):
            to = flip(me_t, j)
            send(
                picked.at[k, pl.ds(pl.multiple_of(to * pad_slot, pad_slot), pad_slot)],
                xin.at[cell(j)], p_send, p_recv.at[k // quarter], me_e, to,
            )
        xin[cell(0), :] = picked[k, pl.ds(pl.multiple_of(me_t * pad_slot, pad_slot), pad_slot), :]


    def conv_ready():
        for name in ("og", "taps", "ggain"):
            loads[name].wait()

        @pl.when(me_e > 0)
        def _():
            settle(h_recv, ig.at[pl.ds(0, 2 * HALO)])

        @pl.when(me_e == 0)
        def _():
            ig[0:HALO, :] = jnp.zeros((HALO, lanes), BF16)

    def conv(j):
        same = (
            lax.broadcasted_iota(jnp.int32, (lanes, lanes), 0) // GROUP_CH
            == lax.broadcasted_iota(jnp.int32, (lanes, lanes), 1) // GROUP_CH
        ).astype(BF16)
        base = pl.multiple_of(flip(me_t, j) * part, part)
        cstep = 64

        @pl.loop(0, part // cstep)
        def _(i):
            at = pl.multiple_of(base + i * cstep, cstep)
            span = pl.ds(at, cstep + HALO)
            product = ig[span, :].astype(F32) * ci[span, :].astype(F32)
            total = taps[reach : reach + 1, :] * product[HALO:, :]
            for back_by in range(1, reach + 1):
                total = total + taps[reach - back_by : reach - back_by + 1, :] * (
                    product[HALO - back_by : HALO - back_by + cstep, :]
                )
            gated[pl.ds(pl.multiple_of(i * cstep, cstep), cstep), :] = (
                og[pl.ds(at, cstep), :].astype(F32) * total
            )

        value = gated[...]
        square = value * value
        s_high = square.astype(BF16)
        s_low = (square - s_high.astype(F32)).astype(BF16)
        mean = (
            jnp.dot(s_high, same, preferred_element_type=F32)
            + jnp.dot(s_low, same, preferred_element_type=F32)
        ) * (1.0 / GROUP_CH)
        done = (value * lax.rsqrt(mean + 1e-06) * ggain[...]).astype(BF16)
        if j:
            normed[pl.ds(base, part), :] = done
        else:
            mixin[0] = done

    def mix_send(j):
        to = flip(me_t, j)
        send(
            normed.at[pl.ds(pl.multiple_of(to * part, part), part)], mixin.at[j],
            m_send, m_recv, me_e, to,
        )

    def mixer():
        settle(m_recv, mixin.at[pl.ds(1, n_tp - 1)])

        for f in range(width // 512):
            cols = pl.ds(f * 512, 512)
            total = jnp.zeros((part, 512), F32)
            for j in range(n_tp):
                depth = pl.ds(pl.multiple_of(flip(me_t, j) * lanes, lanes), lanes)
                total = total + jnp.dot(mixin[j], wm[depth, cols], preferred_element_type=F32)
            mixed[:, cols] = total.astype(BF16)

    hid = wg.shape[1]
    mine = pl.ds(pl.multiple_of(me_t * pad_slot, pad_slot), pad_slot)
    here = pl.ds(pl.multiple_of(me_e * rows, rows), rows)

    def rows_in(ks):
        settle(p_recv.at[ks[0] // quarter], xin.at[pl.ds(ks[0] * slots, len(ks) * (n_tp - 1) * pad_slot)])

    def expert(ks):
        first, count = ks[0], len(ks)
        span = pl.ds(first * slots, count * slots)
        hid_rows = pl.ds(0, count * slots)

        for f in range(hid // 256):
            cols = pl.ds(f * 256, 256)
            gate = jnp.dot(xin[span, :], wg[:, cols], preferred_element_type=F32)
            up = jnp.dot(xin[span, :], wu[:, cols], preferred_element_type=F32)
            hidden[hid_rows, cols] = (gate / (1.0 + jnp.exp(-gate)) * up).astype(BF16)

        for f in range(width // 512):
            cols = pl.ds(f * 512, 512)
            xin[span, cols] = jnp.dot(
                hidden[hid_rows, :], wd[:, cols], preferred_element_type=F32
            ).astype(BF16)

    def give_back(ks):
        for k in ks:
            for j in range(n_tp - 1, 0, -1):
                send(
                    xin.at[pl.ds((k * n_tp + j) * pad_slot, pad_slot)],
                    comb.at[k, mine], r_send, r_recv.at[k], me_e, flip(me_t, j),
                )
            comb[k, mine, :] = xin[pl.ds(k * slots, pad_slot), :]


    def combine(k):
        settle(r_recv.at[k], comb.at[k, others])
        total = jnp.dot(
            landed[k, :, pl.ds(width, slots)], comb[k], preferred_element_type=F32
        ) + jnp.dot(
            landed[k, :, pl.ds(width + slots, slots)], comb[k], preferred_element_type=F32
        )
        if k == 0:
            fin[here, :] = total.astype(BF16)
            return
        sums[k] = total.astype(BF16)
        send(sums.at[k], fin.at[here], f_send, f_recv, flip(me_e, k), me_t)

    half = n_ep // 2
    for step in range(quarter):
        depart(step)
    scatter(0)
    for step in range(quarter + 1, n_ep):
        prepare(step)
        depart(step)
    conv_ready()
    conv(n_tp - 1)
    mix_send(n_tp - 1)
    for j in range(n_tp - 2, -1, -1):
        conv(j)
    mix_send(1)
    for k in q0[1:]:
        scatter(k)
    for k in q1[:split]:
        scatter(k)
    for k in q1[split:]:
        scatter(k)
    for k in q2[:split]:
        scatter(k)
    for name in ("wg", "wu", "wd"):
        loads[name].wait()
    rows_in(q0)
    for k in q2[split:]:
        scatter(k)
    for j in range(n_tp - 2, 1, -1):
        mix_send(j)
    rows_in(q2)
    for k in q3[:split]:
        scatter(k)
    expert(q2)
    give_back(q2[:split])
    rows_in(q1)
    for k in q3[split:]:
        scatter(k)
    give_back(q2[split:])
    expert(q1)
    give_back(q1[split:])
    for k in q2[:split]:
        combine(k)
    loads["wm"].wait()
    mixer()
    rows_in(q3)
    expert(q3)
    for k in q2[split:]:
        combine(k)
    give_back(q3[split:])
    for k in q1[split:]:
        combine(k)
    give_back(q3[:split])
    give_back(q1[:split])
    for k in q3[split:]:
        combine(k)
    expert(q0)
    give_back(q0[split:])
    for k in q3[:split]:
        combine(k)
    give_back(q0[:split])
    for k in q1[:split]:
        combine(k)
    for k in q0[split:]:
        combine(k)
    for k in q0[:split]:
        combine(k)
    settle(f_recv, fin.at[pl.ds(0, (n_ep - 1) * rows)])
    @pl.when(me_e < n_ep - 1)
    def _():
        settle(h_send, ig.at[pl.ds(0, 2 * HALO)])

    settle(d_send, sorted_rows.at[pl.ds(0, (n_ep - 1) * rows)])
    settle(m_send, normed.at[pl.ds(0, (n_tp - 1) * part)])
    settle(p_send, picked.at[:, others])
    settle(r_send, comb.at[:, others])
    settle(f_send, sums.at[pl.ds(0, n_ep - 1)])


def layer(
    out_gate, in_gate, conv_input, conv_taps, group_gain, mix_out_w,
    moe_in, moe_gain, route_ids, route_weight, gate_w, up_w, down_w,
):
    n_ep, n_tp = lax.axis_size("ep"), lax.axis_size("tp")
    tok, width = moe_in.shape
    hid = gate_w.shape[2]
    pad_slot = round_up(2 * tok // (n_ep * n_tp), 16)
    rows = tok // n_ep
    slots = n_tp * pad_slot
    meta = round_up(2 * slots, 128)
    total = n_ep * slots
    rows_a, lanes = out_gate.shape
    part = rows_a // n_tp
    channels = mix_out_w.shape[0]
    taps = conv_taps.shape[0]
    hbm = pl.BlockSpec(memory_space=pltpu.HBM)
    dma = pltpu.SemaphoreType.DMA
    vm = pltpu.VMEM
    scratch = [
        vm((rows_a, lanes), BF16),
        vm((HALO + rows_a, lanes), BF16),
        vm((HALO + rows_a, lanes), BF16),
        vm((taps, lanes), F32),
        vm((1, lanes), F32),
        vm((channels, width), BF16),
        vm((tok, width), BF16),
        vm((1, width), F32),
        vm((2, tok), jnp.int32),
        vm((2, tok), F32),
        vm((width, hid), BF16),
        vm((width, hid), BF16),
        vm((hid, width), BF16),
        vm((rows_a, lanes), BF16),
        vm((part, lanes), F32),
        vm((tok, width), BF16),
        vm((tok, width + meta), BF16),
        vm((n_ep, rows, width + meta), BF16),
        vm((n_ep, slots, width), BF16),
        vm((total, width), BF16),
        vm((total // 4, hid), BF16),
        vm((n_ep, slots, width), BF16),
        vm((n_ep, rows, width), BF16),
        vm((n_tp, part, lanes), BF16),
        dma((13,)),
        dma(()),
        dma(()),
        dma(()),
        dma(()),
        dma(()),
        dma((n_ep,)),
        dma(()),
        dma((4,)),
        dma(()),
        dma((n_ep,)),
        dma(()),
        dma(()),
    ]
    held = 2 * (part * width + tok * width + tok * tok) + sum(
        math.prod(one.shape) * jnp.dtype(one.dtype).itemsize for one in scratch if one.memory_space == vm
    )
    return pl.pallas_call(
        functools.partial(layer_kernel, n_ep, n_tp, pad_slot, taps - 1),
        out_shape=[
            jax.ShapeDtypeStruct((part, width), BF16),
            jax.ShapeDtypeStruct((tok, width), BF16),
            jax.ShapeDtypeStruct((tok, tok), BF16),
        ],
        in_specs=[hbm] * 13,
        out_specs=[pl.BlockSpec(memory_space=vm)] * 3,
        scratch_shapes=scratch,
        compiler_params=pltpu.CompilerParams(
            collective_id=0, has_side_effects=True, vmem_limit_bytes=min(held + SPARE, VMEM_BYTES)
        ),
        cost_estimate=pl.CostEstimate(
            flops=6 * total * width * hid, bytes_accessed=8 * width * hid, transcendentals=0
        ),
    )(*[pltpu.with_memory_space_constraint(a, pltpu.HBM) for a in (
        out_gate, in_gate, conv_input, conv_taps, group_gain.reshape(1, lanes), mix_out_w,
        moe_in, moe_gain.reshape(1, width), route_ids.T, route_weight.T, gate_w, up_w, down_w,
    )])


def finish_kernel(mixed_in, fin, place, mixed, out, done, sem):
    copies = [pltpu.make_async_copy(mixed_in, mixed, sem.at[0])]
    copies[0].start()
    block = 512
    for i in range(done.shape[1] // block):
        cols = pl.ds(i * block, block)
        done[:, cols] = tdot(place[...], fin[:, cols]).astype(BF16)
        copies.append(pltpu.make_async_copy(done.at[:, cols], out.at[:, cols], sem.at[1 + i]))
        copies[-1].start()
    for copy in copies:
        copy.wait()


def shards(*args):
    mixed, fin, place = layer(*args)
    tok, width = fin.shape
    vm = pl.BlockSpec(memory_space=pltpu.VMEM)
    hbm = pl.BlockSpec(memory_space=pl.ANY)
    return pl.pallas_call(
        finish_kernel,
        out_shape=[
            jax.ShapeDtypeStruct(mixed.shape, BF16),
            jax.ShapeDtypeStruct((tok, width), BF16),
        ],
        in_specs=[vm, vm, vm],
        out_specs=[hbm, hbm],
        scratch_shapes=[pltpu.VMEM((tok, width), BF16), pltpu.SemaphoreType.DMA((1 + width // 512,))],
        compiler_params=pltpu.CompilerParams(vmem_limit_bytes=8 << 20),
        cost_estimate=pl.CostEstimate(
            flops=2 * tok * tok * width, bytes_accessed=8 * tok * width, transcendentals=0
        ),
    )(mixed, fin, place)


def solution(mesh):
    in_specs = (
        P("ep", "tp"),
        P("ep", "tp"),
        P("ep", "tp"),
        P(None, "tp"),
        P("tp"),
        P(),
        P(("ep", "tp"), None),
        P(),
        P(("ep", "tp"), None),
        P(("ep", "tp"), None),
        P(("ep", "tp"), None, None),
        P(("ep", "tp"), None, None),
        P(("ep", "tp"), None, None),
    )
    out_specs = (P(("ep", "tp"), None), P(("ep", "tp"), None))
    return jax.shard_map(shards, mesh=mesh, in_specs=in_specs, out_specs=out_specs, check_vma=False)
```
